32 devices in a mesh: sp: 4 (over y, x), tp: 8 (over z, core).
Axes of the slice: x: 2, y: 2, z: 4, core: 2. Of those that a mesh axis runs over, the one named last changes fastest.
Arguments:
- moe_input: bfloat16 [512, 2048], P('sp'), may hold values from -6 to 6
- cotangent: bfloat16 [512, 2048], P('sp'), may hold values from -6 to 6
- route_expert: int32 [512, 2], P('sp'), may hold values from 0 to 3, all different within a row; in each aligned block of 128 rows (0 to 127, 128 to 255, ...) at most 128 rows name the same one
- route_weight: float32 [512, 2], P('sp'), may hold values from 0.2 to 1
- w_gate: bfloat16 [4, 2048, 6144], P('sp', None, 'tp'), may hold values from -0.125 to 0.125
- w_up: bfloat16 [4, 2048, 6144], P('sp', None, 'tp'), may hold values from -0.125 to 0.125
- w_down: bfloat16 [4, 6144, 2048], P('sp', 'tp'), may hold values from -0.078125 to 0.078125
- out_proj: bfloat16 [2048, 2048], P('tp'), may hold values from -0.125 to 0.125
- saved_out: bfloat16 [512, 2048], P('sp', 'tp'), may hold values from -6 to 6
- queries: bfloat16 [512, 1024], P('sp', 'tp'), may hold values from -6 to 6
- keys: bfloat16 [512, 1024], P('sp', 'tp'), may hold values from -6 to 6
- values: bfloat16 [512, 2048], P('sp', 'tp'), may hold values from -6 to 6
- log_decay: float32 [512, 1024], P('sp', 'tp'), may hold values from -1 to 0
- span_state: float32 [8, 1024, 128], P('sp', 'tp'), may hold values from -6 to 6
Outputs:
- grad_w_gate: bfloat16 [4, 2048, 6144], P('sp', None, 'tp')
- grad_w_up: bfloat16 [4, 2048, 6144], P('sp', None, 'tp')
- grad_w_down: bfloat16 [4, 6144, 2048], P('sp', 'tp')
- grad_proj: float32 [2048, 2048], P('sp', 'tp')
- grad_queries: bfloat16 [512, 1024], P('sp', 'tp')
- grad_keys: bfloat16 [512, 1024], P('sp', 'tp')
- grad_values: bfloat16 [512, 2048], P('sp', 'tp')
- grad_decay: float32 [512, 1024], P('sp', 'tp')
The draws below stay inside these ranges and needn't reach their ends.
Inputs may be any that keep to these rules, and one draw needn't show every extreme that they name: `route_expert`: each row names two different experts. Within the 128 rows of one index of sp no expert is named by more than 128 rows, a bound that some block reaches.
All inputs are finite; a program needn't handle non-finite values.
Results may differ from the reference program's by a relative error of at most 0.019.
Values may be sent and summed in bfloat16 or wider, within the bound.
No kernel may reach another device: no remote copies, remote signals or barrier semaphores. Data moves between devices by JAX's collectives and lax.ppermute only.
A program may use at most 128 MiB of HBM per device.

```python
import math
import jax
import jax.numpy as jnp
import numpy as np
from jax import lax

D = 2048
HEADS = 16
DK = 64
DV = 128
F = 6144
SPAN = 64
TOK_DEV = 128
TOKENS = 512
EXPERTS = 4
CAP = 128
N_SP = 4


def draw_log_decay(key, part):
    keys_list = jax.random.split(jax.random.fold_in(key, 11), 7)
    channels = HEADS * DK
    fast_variant = jax.random.uniform(keys_list[0], (channels,)) < 0.5
    slow_rate = jnp.log(10.0) / TOKENS * jax.random.uniform(keys_list[1], (channels,), minval=0.1, maxval=0.4)
    quick_rate = 1.0 / jax.random.uniform(keys_list[2], (channels,), minval=30.0, maxval=50.0)
    starting_offset = jnp.where(fast_variant, quick_rate, slow_rate)
    coarse_estimate = jnp.exp(jax.random.uniform(keys_list[3], (TOKENS, channels), minval=-0.7, maxval=0.7))
    levels = jax.random.uniform(keys_list[4], (TOKENS // TOK_DEV, 1, 1), minval=-0.7, maxval=0.7)
    block_multiplier = jnp.exp(jnp.broadcast_to(levels, (TOKENS // TOK_DEV, TOK_DEV, 1)).reshape(TOKENS, 1))
    target_locations = jax.random.randint(keys_list[5], (3,), 0, TOKENS)
    token_locations = jnp.arange(TOKENS, dtype=jnp.int32)
    transfer_group_rows = jnp.any(token_locations[:, None] == target_locations[None, :], axis=1).astype(jnp.float32)
    layer_stack_depth = -jnp.log(jax.random.uniform(keys_list[6], (channels,), minval=0.5, maxval=0.8))
    transfer_group = transfer_group_rows[:, None] * jnp.where(fast_variant, 0.0, layer_stack_depth)[None, :]
    return (-(starting_offset[None, :] * coarse_estimate * block_multiplier) - transfer_group).astype(jnp.float32)


def raised(values, rng, source, target, shards_of, factor):
    owner, partner = [(jnp.arange(values.shape[position]) // (values.shape[position] // shards_of)).reshape([-1 if axis == position else 1 for axis in range(values.ndim)]) for position in (source, target)]
    chosen = jax.random.permutation(rng, shards_of)[partner]
    strong = (owner == chosen) | (owner == (partner + shards_of // 2) % shards_of)
    return jnp.where(strong, factor * values, values)


def shard_levels(stream_key, dims, cuts, low, top_value):
    gain, own = 1.0, jax.random.fold_in(stream_key, 6)
    for position, blocks in cuts:
        heights = jnp.exp(jax.random.uniform(jax.random.fold_in(own, position), (blocks,), jnp.float32, low / len(cuts), top_value / len(cuts)))
        gain = gain * jnp.repeat(heights, dims[position] // blocks).reshape([-1 if axis == position else 1 for axis in range(len(dims))])
    return gain


def routed_block(own_key, own, number, rows, count, top, limit, slope):
    ranking = jax.random.permutation(own_key, count)
    crowded, ordinary = portions_of(count, rows * top, limit, slope, True), portions_of(count, rows * top, limit, slope, False)
    places = jnp.arange(count)

    def named(lengths, offset_by):
        used = int((lengths > 0).sum())
        fixed = max(1, used // 4)
        moved = fixed + (places - fixed + offset_by * (used - fixed)) % max(1, count - fixed)
        return jnp.zeros((count,), jnp.int32).at[ranking[jnp.where(places < fixed, places, moved)]].set(jnp.asarray(lengths, jnp.int32))

    lengths = jnp.where(number % 4 == 0, named(crowded, number // 4), named(ordinary, number - number // 4 - 1))
    mixed = jax.random.permutation(jax.random.fold_in(own, 3), count)
    source_of, taker = mixed[0:count // 2 * 2:2], mixed[1:count // 2 * 2:2]
    room = jnp.minimum(lengths[source_of] - 1, limit - lengths[taker]) // 2
    room = jnp.where((source_of == ranking[0]) | (taker == ranking[0]) | (lengths[taker] == 0), 0, jnp.maximum(room, 0))
    moved = jax.random.randint(jax.random.fold_in(own, 4), (count // 2,), 0, 1 << 20) % (room + 1)
    lengths = lengths.at[source_of].add(-moved).at[taker].add(moved)
    items = jnp.searchsorted(jnp.cumsum(lengths), jnp.arange(rows * top), side="right").astype(jnp.int32)
    table = items.reshape(top, rows).T
    table = table[jax.random.permutation(jax.random.fold_in(own, 1), rows)]
    offset_by = jax.random.randint(jax.random.fold_in(own, 2), (rows, 1), 0, top)
    return jnp.take_along_axis(table, (jnp.arange(top)[None, :] + offset_by) % top, axis=1)


def portions_of(count, total, bound, lean, full):
    loads = [(1 << 20) // math.isqrt(standing ** lean) + 1 for standing in range(1, count + 1)]
    largest = bound if full else min(bound, max(-(-total // count), total * loads[0] // sum(loads)))
    least = 1 if total - largest >= count - 1 else 0
    holding, spare = [largest] + [least] * (count - 1), total - largest - least * (count - 1)
    while spare > 0:
        free = [i for i in range(1, count) if holding[i] < largest] or [i for i in range(1, count) if holding[i] < bound]
        whole, left = sum([loads[i] for i in free]), spare
        for i in free:
            extra = min(bound - holding[i], max(1, left * loads[i] // whole), spare)
            holding[i] = holding[i] + extra
            spare = spare - extra
    return np.array(holding)


def normal_values(rng, extent, spread, most, shards=(), kind=jnp.bfloat16):
    drawn = spread * jax.random.normal(rng, extent, jnp.float32)
    if shards:
        drawn = drawn * shard_levels(rng, extent, shards, -0.22, 0.18)
    return jnp.clip(drawn, -most, most).astype(kind)


def bell_draw_with(own_key, shape, scale, most, cuts, heavy, held_as=jnp.bfloat16):
    values = scale * jax.random.normal(own_key, shape, jnp.float32)
    if cuts:
        values = values * shard_levels(own_key, shape, cuts, -0.22, 0.18)
    return jnp.clip(raised(values, jax.random.fold_in(own_key, 3), *heavy), -most, most).astype(held_as)


def setup_inputs(seed: int = 0) -> dict:
    seeds = jax.random.split(jax.random.key(seed), 15)
    moe_input = normal_values(seeds[0], (TOKENS, D), 1.0, 6.0, ((0, 4),))
    cotangent = bell_draw_with(seeds[1], (TOKENS, D), 1.0, 6.0, ((0, 4),), (0, 1, 4, 2.0))
    route_expert_keys = jax.random.split(jax.random.fold_in(seeds[2], 1), TOKENS // TOK_DEV)
    route_expert_turns = jax.random.permutation(jax.random.fold_in(seeds[2], 3), TOKENS // TOK_DEV)
    route_expert = jax.vmap(lambda own, number: routed_block(jax.random.fold_in(seeds[2], 2), own, number, TOK_DEV, EXPERTS, 2, CAP, 1))(route_expert_keys, route_expert_turns).reshape((TOKENS, 2))
    route_weight = jnp.clip(0.2 + 0.8 * jax.random.uniform(seeds[3], (TOKENS, 2), jnp.float32) ** shard_levels(seeds[3], (TOKENS, 2), ((0, 4),), -0.2, 0.2), 0.2, 1.0)
    w_gate = normal_values(seeds[4], (EXPERTS, D, F), D ** -0.5, 0.125, ((0, 4), (2, 8)))
    w_up = normal_values(seeds[5], (EXPERTS, D, F), D ** -0.5, 0.125, ((0, 4), (2, 8)))
    w_down = normal_values(seeds[6], (EXPERTS, F, D), F ** -0.5, 0.078125, ((0, 4), (1, 8)))
    out_proj = normal_values(seeds[7], (HEADS * DV, D), (HEADS * DV) ** -0.5, 0.125, ((0, 8),))
    saved_out = normal_values(seeds[8], (TOKENS, HEADS * DV), 1.0, 6.0, ((0, 4), (1, 8)))
    queries = normal_values(seeds[9], (TOKENS, HEADS * DK), 1.0, 6.0, ((0, 4), (1, 8)))
    keys = normal_values(seeds[10], (TOKENS, HEADS * DK), 1.0, 6.0, ((0, 4), (1, 8)))
    values = normal_values(seeds[11], (TOKENS, HEADS * DV), 1.0, 6.0, ((0, 4), (1, 8)))
    log_decay = draw_log_decay(jax.random.fold_in(seeds[14], 71), 0)
    span_state = normal_values(seeds[13], (TOKENS // SPAN, HEADS * DK, DV), 1.0, 6.0, ((0, 4), (1, 8)), jnp.float32)
    return {"moe_input": moe_input, "cotangent": cotangent, "route_expert": route_expert, "route_weight": route_weight, "w_gate": w_gate, "w_up": w_up, "w_down": w_down, "out_proj": out_proj, "saved_out": saved_out, "queries": queries, "keys": keys, "values": values, "log_decay": log_decay, "span_state": span_state}


HIGH = lax.Precision.HIGHEST

def slot_places(experts, count):
    routes_flat = experts.reshape(-1)
    one_hot = (routes_flat[:, None] == jnp.arange(count, dtype=jnp.int32)[None, :]).astype(jnp.int32)
    earlier = jnp.cumsum(one_hot, axis=0) - one_hot
    return lax.optimization_barrier(jnp.sum(earlier * one_hot, axis=1)).reshape(experts.shape).astype(jnp.int32)

def expert_grads(inputs, routed, gate_weight, up_weight, down_weight):
    gate = jnp.dot(inputs, gate_weight, preferred_element_type=jnp.float32)
    upper = jnp.dot(inputs, up_weight, preferred_element_type=jnp.float32)
    sigmoid_gate = jax.nn.sigmoid(gate)
    active = gate * sigmoid_gate
    hidden = (active * upper).astype(jnp.bfloat16)
    d_hidden = lax.dot_general(routed, down_weight, (((1,), (1,)), ((), ())), preferred_element_type=jnp.float32)
    d_upper = (d_hidden * active).astype(jnp.bfloat16)
    d_gate = (d_hidden * upper * sigmoid_gate * (1.0 + gate * (1.0 - sigmoid_gate))).astype(jnp.bfloat16)
    grad_down = lax.dot_general(hidden, routed, (((0,), (0,)), ((), ())), preferred_element_type=jnp.float32).astype(jnp.bfloat16)
    grad_gate = lax.dot_general(inputs, d_gate, (((0,), (0,)), ((), ())), preferred_element_type=jnp.float32).astype(jnp.bfloat16)
    grad_up = lax.dot_general(inputs, d_upper, (((0,), (0,)), ((), ())), preferred_element_type=jnp.float32).astype(jnp.bfloat16)
    return (d_gate, d_upper, grad_gate, grad_up, grad_down)

def input_grad(d_gate, d_upper, gate_weight, up_weight):
    first = lax.dot_general(d_gate, gate_weight, (((1,), (1,)), ((), ())), preferred_element_type=jnp.float32)
    second = lax.dot_general(d_upper, up_weight, (((1,), (1,)), ((), ())), preferred_element_type=jnp.float32)
    return first + second

def gated_pieces(queries, keys, values, log_decay, grad_mix, key_dim, span_len):
    value_dim = values.shape[1] * key_dim // queries.shape[1]
    heads = queries.shape[1] // key_dim
    spans = queries.shape[0] // span_len

    def blocks(array, width):
        return array.astype(jnp.float32).reshape(spans, span_len, heads, width)
    query_spans = blocks(queries, key_dim)
    key_spans = blocks(keys, key_dim)
    value_spans = blocks(values, value_dim)
    grad_spans = blocks(grad_mix, value_dim)
    cumulative = jnp.cumsum(blocks(log_decay, key_dim), axis=1)
    last = cumulative[:, -1]
    scale = key_dim ** (-0.5)
    query_decayed = query_spans * jnp.exp(cumulative)
    key_grown = key_spans * jnp.exp(-cumulative)
    key_to_end = key_spans * jnp.exp(last[:, None] - cumulative)
    g_local = scale * jnp.einsum('nthk,nthv->nhkv', query_decayed, grad_spans, precision=HIGH)
    return (query_spans, key_spans, value_spans, grad_spans, cumulative, last, query_decayed, key_grown, key_to_end, g_local)

def backward_step(carry, inputs):
    local, decay = inputs
    return (local + jnp.exp(decay)[..., None] * carry, carry)

def gated_finish(pieces, span_state, g_end, key_dim):
    query_spans, key_spans, value_spans, grad_spans, cumulative, last, query_decayed, key_grown, key_to_end, g_local = pieces
    spans, span_len, heads, value_dim = value_spans.shape
    scale = key_dim ** (-0.5)
    token_locations = jnp.arange(span_len, dtype=jnp.int32)
    causal = (token_locations[:, None] >= token_locations[None, :]).astype(jnp.float32)
    scores = jnp.einsum('nthk,nshk->nhts', query_decayed, key_grown, precision=HIGH) * causal
    grad_dot = jnp.einsum('nthv,nshv->nhts', grad_spans, value_spans, precision=HIGH) * causal
    state = span_state.astype(jnp.float32).reshape(spans, heads, key_dim, value_dim)
    d_query = scale * jnp.exp(cumulative) * (jnp.einsum('nhts,nshk->nthk', grad_dot, key_grown, precision=HIGH) + jnp.einsum('nthv,nhkv->nthk', grad_spans, state, precision=HIGH))
    d_key = scale * jnp.exp(-cumulative) * jnp.einsum('nhts,nthk->nshk', grad_dot, query_decayed, precision=HIGH) + jnp.exp(last[:, None] - cumulative) * jnp.einsum('nshv,nhkv->nshk', value_spans, g_end, precision=HIGH)
    d_value = scale * jnp.einsum('nhts,nthv->nshv', scores, grad_spans, precision=HIGH) + jnp.einsum('nshk,nhkv->nshv', key_to_end, g_end, precision=HIGH)
    state_end = jnp.exp(last)[..., None] * state + jnp.einsum('nshk,nshv->nhkv', key_to_end, value_spans, precision=HIGH)
    tail = lax.optimization_barrier(jnp.sum(state_end * g_end, axis=-1))
    d_cumulative = query_spans * d_query - key_spans * d_key
    d_log = jnp.cumsum(d_cumulative[:, ::-1], axis=1)[:, ::-1] + tail[:, None]
    rows = spans * span_len
    return (d_query.reshape(rows, heads * key_dim).astype(jnp.bfloat16), d_key.reshape(rows, heads * key_dim).astype(jnp.bfloat16), d_value.reshape(rows, heads * value_dim).astype(jnp.bfloat16), d_log.reshape(rows, heads * key_dim))

def place_block(block):
    return slot_places(block, EXPERTS)

def per_expert(items):
    rows_in, rows_cot, gate_weight, up_weight, down_weight = items
    d_gate, d_upper, grad_gate, grad_up, grad_down = expert_grads(rows_in, rows_cot, gate_weight, up_weight, down_weight)
    return (input_grad(d_gate, d_upper, gate_weight, up_weight), grad_gate, grad_up, grad_down)

def reference(moe_input, cotangent, route_expert, route_weight, w_gate, w_up, w_down, out_proj, saved_out, queries, keys, values, log_decay, span_state):
    blocks = route_expert.reshape(N_SP, TOK_DEV, 2)
    target_locations = jax.vmap(place_block)(blocks)
    source = jnp.arange(N_SP, dtype=jnp.int32)[:, None, None]
    slot_index = (blocks * (N_SP * CAP) + source * CAP + target_locations).reshape(-1).astype(jnp.int32)
    owner = jnp.full((EXPERTS * N_SP * CAP,), 2 * TOKENS, jnp.int32).at[slot_index].set(jnp.arange(2 * TOKENS, dtype=jnp.int32))
    weighted = (route_weight[:, :, None] * cotangent[:, None, :].astype(jnp.float32)).astype(jnp.bfloat16)
    weighted = weighted.reshape(2 * TOKENS, D)
    blank = jnp.zeros((1, D), jnp.bfloat16)
    slot_cot = jnp.concatenate([weighted, blank], axis=0)[owner].reshape(EXPERTS, N_SP * CAP, D)
    slot_in = jnp.concatenate([moe_input, blank], axis=0)[owner // 2].reshape(EXPERTS, N_SP * CAP, D)
    slot_grad, grad_w_gate, grad_w_up, grad_w_down = lax.map(per_expert, (slot_in, slot_cot, w_gate, w_up, w_down))
    routed = slot_grad.reshape(-1, D)[slot_index].reshape(TOKENS, 2, D)
    grad_in = (cotangent.astype(jnp.float32) + routed[:, 0] + routed[:, 1]).astype(jnp.bfloat16)
    grad_mix = lax.dot_general(grad_in, out_proj, (((1,), (1,)), ((), ())), preferred_element_type=jnp.float32)
    grad_proj = lax.dot_general(grad_in, saved_out, (((0,), (0,)), ((), ())), preferred_element_type=jnp.float32)
    pieces = gated_pieces(queries, keys, values, log_decay, grad_mix, DK, SPAN)
    g_local = pieces[9]
    last = pieces[5]
    begin = jnp.zeros((HEADS, DK, DV), jnp.float32)
    ignored, g_end = lax.scan(backward_step, begin, (g_local, last), reverse=True)
    grad_queries, grad_keys, grad_values, grad_decay = gated_finish(pieces, span_state, g_end, DK)
    return (grad_w_gate, grad_w_up, grad_w_down, grad_proj, grad_queries, grad_keys, grad_values, grad_decay)
```

```python
import functools

import jax
import jax.numpy as jnp
from jax import lax
from jax.experimental import pallas as pl
from jax.experimental.pallas import tpu as pltpu
from jax.sharding import PartitionSpec as P

DK = 64
SPAN = 64
HIGH = lax.Precision.HIGHEST
BF = jnp.bfloat16
F32 = jnp.float32


VM = pl.BlockSpec(memory_space=pltpu.VMEM)
SM = pl.BlockSpec(memory_space=pltpu.SMEM)


def entering(shard, axis, combine, identity):
    length, mine = (lax.axis_size(axis), lax.axis_index(axis))
    everything = jax.tree.map(lambda part: lax.all_gather(part, axis), shard)
    start = jax.tree.map(
        lambda part, zero: jnp.broadcast_to(jnp.asarray(zero, part.dtype), part.shape),
        shard,
        identity,
    )

    def step(k, before):
        at = length - 1 - k
        reached = at > mine
        new = combine(before, jax.tree.map(lambda part: part[at], everything))
        return jax.tree.map(lambda a, b: jnp.where(reached, a, b), new, before)

    return lax.fori_loop(0, length, step, start)


def slot_places(experts, count):
    routes_flat = experts.reshape(-1)
    one_hot = (routes_flat[:, None] == jnp.arange(count, dtype=jnp.int32)[None, :]).astype(
        jnp.int32
    )
    earlier = jnp.cumsum(one_hot, axis=0) - one_hot
    return jnp.sum(earlier * one_hot, axis=1).reshape(experts.shape)


def expert_grads(inputs, routed, gate_weight, up_weight, down_weight):
    gate = jnp.dot(inputs, gate_weight, preferred_element_type=jnp.float32)
    upper = jnp.dot(inputs, up_weight, preferred_element_type=jnp.float32)
    sigmoid_gate = jax.nn.sigmoid(gate)
    active = gate * sigmoid_gate
    hidden = (active * upper).astype(jnp.bfloat16)
    d_hidden = lax.dot_general(
        routed, down_weight, (((1,), (1,)), ((), ())), preferred_element_type=jnp.float32
    )
    d_upper = (d_hidden * active).astype(jnp.bfloat16)
    d_gate = (d_hidden * upper * sigmoid_gate * (1.0 + gate * (1.0 - sigmoid_gate))).astype(
        jnp.bfloat16
    )
    grad_down = lax.dot_general(
        hidden, routed, (((0,), (0,)), ((), ())), preferred_element_type=jnp.float32
    ).astype(jnp.bfloat16)
    grad_gate = lax.dot_general(
        inputs, d_gate, (((0,), (0,)), ((), ())), preferred_element_type=jnp.float32
    ).astype(jnp.bfloat16)
    grad_up = lax.dot_general(
        inputs, d_upper, (((0,), (0,)), ((), ())), preferred_element_type=jnp.float32
    ).astype(jnp.bfloat16)
    return (d_gate, d_upper, grad_gate, grad_up, grad_down)


def input_grad(d_gate, d_upper, gate_weight, up_weight):
    first = lax.dot_general(
        d_gate, gate_weight, (((1,), (1,)), ((), ())), preferred_element_type=jnp.float32
    )
    second = lax.dot_general(
        d_upper, up_weight, (((1,), (1,)), ((), ())), preferred_element_type=jnp.float32
    )
    return first + second


def gated_pieces(queries, keys, values, log_decay, grad_mix, key_dim, span_len):
    value_dim = values.shape[1] * key_dim // queries.shape[1]
    heads = queries.shape[1] // key_dim
    spans = queries.shape[0] // span_len

    def blocks(array, width):
        return array.astype(jnp.float32).reshape(spans, span_len, heads, width)

    query_spans = blocks(queries, key_dim)
    key_spans = blocks(keys, key_dim)
    value_spans = blocks(values, value_dim)
    grad_spans = blocks(grad_mix, value_dim)
    cumulative = jnp.cumsum(blocks(log_decay, key_dim), axis=1)
    last = cumulative[:, -1]
    scale = key_dim ** (-0.5)
    query_decayed = query_spans * jnp.exp(cumulative)
    key_grown = key_spans * jnp.exp(-cumulative)
    key_to_end = key_spans * jnp.exp(last[:, None] - cumulative)
    g_local = scale * jnp.einsum("nthk,nthv->nhkv", query_decayed, grad_spans, precision=HIGH)
    return (
        query_spans,
        key_spans,
        value_spans,
        grad_spans,
        cumulative,
        last,
        query_decayed,
        key_grown,
        key_to_end,
        g_local,
    )


def backward_step(carry, inputs):
    local, decay = inputs
    return (local + jnp.exp(decay)[..., None] * carry, carry)


def gated_finish(pieces, span_state, g_end, key_dim):
    (
        query_spans,
        key_spans,
        value_spans,
        grad_spans,
        cumulative,
        last,
        query_decayed,
        key_grown,
        key_to_end,
        g_local,
    ) = pieces
    spans, span_len, heads, value_dim = value_spans.shape
    scale = key_dim ** (-0.5)
    token_locations = jnp.arange(span_len, dtype=jnp.int32)
    causal = (token_locations[:, None] >= token_locations[None, :]).astype(jnp.float32)
    scores = jnp.einsum("nthk,nshk->nhts", query_decayed, key_grown, precision=HIGH) * causal
    grad_dot = jnp.einsum("nthv,nshv->nhts", grad_spans, value_spans, precision=HIGH) * causal
    state = span_state.reshape(spans, heads, key_dim, value_dim)
    d_query = (
        scale
        * jnp.exp(cumulative)
        * (
            jnp.einsum("nhts,nshk->nthk", grad_dot, key_grown, precision=HIGH)
            + jnp.einsum("nthv,nhkv->nthk", grad_spans, state, precision=HIGH)
        )
    )
    d_key = scale * jnp.exp(-cumulative) * jnp.einsum(
        "nhts,nthk->nshk", grad_dot, query_decayed, precision=HIGH
    ) + jnp.exp(last[:, None] - cumulative) * jnp.einsum(
        "nshv,nhkv->nshk", value_spans, g_end, precision=HIGH
    )
    d_value = scale * jnp.einsum(
        "nhts,nthv->nshv", scores, grad_spans, precision=HIGH
    ) + jnp.einsum("nshk,nhkv->nshv", key_to_end, g_end, precision=HIGH)
    state_end = jnp.exp(last)[..., None] * state + jnp.einsum(
        "nshk,nshv->nhkv", key_to_end, value_spans, precision=HIGH
    )
    tail = jnp.sum(state_end * g_end, axis=-1)
    d_cumulative = query_spans * d_query - key_spans * d_key
    d_log = jnp.cumsum(d_cumulative[:, ::-1], axis=1)[:, ::-1] + tail[:, None]
    rows = spans * span_len
    return (
        d_query.reshape(rows, heads * key_dim).astype(jnp.bfloat16),
        d_key.reshape(rows, heads * key_dim).astype(jnp.bfloat16),
        d_value.reshape(rows, heads * value_dim).astype(jnp.bfloat16),
        d_log.reshape(rows, heads * key_dim),
    )


def carry_combine(earlier, later):
    return (later[0] * earlier[0], later[1] + later[0][..., None] * earlier[1])


def by_slots(
    moe_input,
    cotangent,
    route_expert,
    route_weight,
    w_gate,
    w_up,
    w_down,
    out_proj,
    saved_out,
    queries,
    keys,
    values,
    log_decay,
    span_state,
):
    tok_rows, width = moe_input.shape
    groups = lax.axis_size("sp")
    lanes = lax.axis_size("tp")
    capacity = 4 * tok_rows // groups
    target_locations = slot_places(route_expert, groups)
    rows_index = (target_locations * groups + route_expert).reshape(-1)
    owner = (
        jnp.full((capacity * groups,), 2 * tok_rows, jnp.int32)
        .at[rows_index]
        .set(jnp.arange(2 * tok_rows, dtype=jnp.int32))
    )
    weighted = (route_weight[:, :, None] * cotangent[:, None, :].astype(jnp.float32)).astype(
        jnp.bfloat16
    )
    weighted = weighted.reshape(2 * tok_rows, width)
    blank = jnp.zeros((1, width), jnp.bfloat16)
    send_in = jnp.concatenate([moe_input, blank], axis=0)[owner // 2].reshape(
        capacity, groups, width
    )
    send_cot = jnp.concatenate([weighted, blank], axis=0)[owner].reshape(capacity, groups, width)
    gate_weight = w_gate[0]
    up_weight = w_up[0]
    down_weight = w_down[0]
    share = capacity // lanes
    lane = lax.axis_index("tp")
    part_in = lax.dynamic_slice_in_dim(send_in, lane * share, share, 0)
    part_cot = lax.dynamic_slice_in_dim(send_cot, lane * share, share, 0)
    got_in, got_cot = (
        lax.all_to_all(part_in, "sp", split_axis=1, concat_axis=1, tiled=True),
        lax.all_to_all(part_cot, "sp", split_axis=1, concat_axis=1, tiled=True),
    )
    full_in, full_cot = (
        lax.all_gather(got_in, "tp", axis=0, tiled=True),
        lax.all_gather(got_cot, "tp", axis=0, tiled=True),
    )
    d_gate, d_upper, grad_gate, grad_up, grad_down = expert_grads(
        full_in.reshape(-1, width), full_cot.reshape(-1, width), gate_weight, up_weight, down_weight
    )
    mine = (
        lax.psum_scatter(
            input_grad(d_gate, d_upper, gate_weight, up_weight).astype(jnp.bfloat16),
            "tp",
            scatter_dimension=0,
            tiled=True,
        )
        .astype(jnp.float32)
        .reshape(share, groups, width)
    )
    returned = (
        lax.all_to_all(mine.astype(jnp.bfloat16), "sp", split_axis=1, concat_axis=1, tiled=True)
        .astype(mine.dtype)
        .reshape(-1, width)
    )
    local_index = rows_index - lane * share * groups
    inside = (local_index >= 0) & (local_index < share * groups)
    picked = jnp.where(inside[:, None], returned[jnp.clip(local_index, 0, share * groups - 1)], 0.0)
    routed = jnp.sum(picked.reshape(tok_rows, 2, width), axis=1)
    total = lax.psum(routed.astype(jnp.bfloat16), "tp").astype(jnp.float32)
    grad_in = (cotangent.astype(jnp.float32) + total).astype(jnp.bfloat16)
    grad_mix = lax.dot_general(
        grad_in, out_proj, (((1,), (1,)), ((), ())), preferred_element_type=jnp.float32
    )
    grad_proj = lax.psum_scatter(
        lax.dot_general(
            grad_in, saved_out, (((0,), (0,)), ((), ())), preferred_element_type=jnp.float32
        ).astype(jnp.bfloat16),
        "sp",
        scatter_dimension=0,
        tiled=True,
    ).astype(jnp.float32)
    pieces = gated_pieces(queries, keys, values, log_decay, grad_mix, DK, SPAN)
    g_local = pieces[9]
    last = pieces[5]
    begin = jnp.zeros(g_local.shape[1:], jnp.float32)
    device_start, local_end = lax.scan(backward_step, begin, (g_local, last), reverse=True)
    device_decay = jnp.exp(jnp.sum(last, axis=0))
    identity = (jnp.ones_like(device_decay), jnp.zeros_like(device_start))
    decay_after, state_after = entering((device_decay, device_start), "sp", carry_combine, identity)
    running = jnp.cumsum(last, axis=0)
    beyond = running[-1][None] - running
    g_end = local_end + jnp.exp(beyond)[..., None] * state_after[None]
    grad_queries, grad_keys, grad_values, grad_decay = gated_finish(pieces, span_state, g_end, DK)
    return (
        grad_gate[None],
        grad_up[None],
        grad_down[None],
        grad_proj,
        grad_queries,
        grad_keys,
        grad_values,
        grad_decay,
    )


def nt(a, b):
    return lax.dot_general(a, b, (((1,), (1,)), ((), ())), preferred_element_type=F32)


def nn(a, b):
    return lax.dot_general(a, b, (((1,), (0,)), ((), ())), preferred_element_type=F32)


def swap(value, axis, mask):
    size = lax.axis_size(axis)
    return lax.ppermute(value, axis, [(i, i ^ mask) for i in range(size)])


def two_hops(mask):
    return mask & (mask - 1) != 0


def prep_kernel(groups, shared, where_ref, x_ref, cot_ref, expert_ref, weight_ref, *outs):
    rows = x_ref.shape[0]
    half = rows // 2
    mine, core, level = where_ref[0], where_ref[1], where_ref[2]

    def weight_of(expert, start, count):
        named = expert_ref[pl.ds(start, count), :] == expert
        return jnp.sum(jnp.where(named, weight_ref[pl.ds(start, count), :], 0.0), axis=1, keepdims=True)

    own_ref = outs[-1]
    for at in range(0, rows, half):
        block = pl.ds(at, half)
        own_ref[block, :] = (weight_of(mine, at, half) * cot_ref[block, :].astype(F32)).astype(BF)
    for mask in range(1, groups):
        out = outs[mask - 1]
        count = out.shape[1]
        start = core * half
        if shared[mask]:
            start = start + (level % 2) * count
        start = pl.multiple_of(start, count)
        block = pl.ds(start, count)
        out[0] = x_ref[block, :]
        out[1] = (weight_of(mine ^ mask, start, count) * cot_ref[block, :].astype(F32)).astype(BF)


def prepare(place, x, cot, expert, weight, groups, shared):
    rows, width = x.shape
    shapes = [
        jax.ShapeDtypeStruct((2, rows // 4 if shared[mask] else rows // 2, width), BF)
        for mask in range(1, groups)
    ]
    shapes.append(jax.ShapeDtypeStruct((rows, width), BF))
    return pl.pallas_call(
        functools.partial(prep_kernel, groups, shared),
        out_shape=shapes,
        in_specs=[SM, VM, VM, VM, VM],
        out_specs=[VM] * len(shapes),
        name="prep",
    )(place, x, cot, expert, weight)


def expert_math(x, cot, gate_w, up_w, down_w):
    gate = nn(x, gate_w)
    upper = nn(x, up_w)
    sigmoid = 1.0 / (1.0 + jnp.exp(-gate))
    active = gate * sigmoid
    hidden = (active * upper).astype(BF)
    d_hidden = nt(cot, down_w)
    d_upper = (d_hidden * active).astype(BF)
    d_gate = (d_hidden * upper * sigmoid * (1.0 + gate * (1.0 - sigmoid))).astype(BF)
    grad = nt(d_gate, gate_w) + nt(d_upper, up_w)
    return hidden, d_gate, d_upper, grad


def own_kernel(where_ref, x_ref, cot_ref, gate_ref, up_ref, down_ref, hid_ref, dg_ref, du_ref, out_ref):
    step = pl.program_id(0)
    hid_ref[...], dg_ref[...], du_ref[...], grad = expert_math(
        x_ref[...], cot_ref[...], gate_ref[...], up_ref[...], down_ref[...]
    )

    @pl.when(step == 0)
    def _():
        out_ref[...] = grad

    @pl.when(step != 0)
    def _():
        out_ref[...] += grad


def tile_of(hidden):
    return 256 if hidden % 256 == 0 else 128


def own_rows(place, x, cot, gate_w, up_w, down_w):
    rows, width = x.shape
    hidden = gate_w.shape[1]
    tile = tile_of(hidden)
    whole = pl.BlockSpec((rows, width), lambda f: (0, 0))
    col = pl.BlockSpec((rows, tile), lambda f: (0, f))
    return pl.pallas_call(
        own_kernel,
        grid=(hidden // tile,),
        out_shape=[jax.ShapeDtypeStruct((rows, hidden), BF)] * 3 + [jax.ShapeDtypeStruct((rows, width), F32)],
        in_specs=[
            SM, whole, whole,
            pl.BlockSpec((width, tile), lambda f: (0, f)),
            pl.BlockSpec((width, tile), lambda f: (0, f)),
            pl.BlockSpec((tile, width), lambda f: (f, 0)),
        ],
        out_specs=[col] * 3 + [whole],
        compiler_params=pltpu.CompilerParams(vmem_limit_bytes=60 * 1024 * 1024),
        name="own_rows",
    )(place, x, cot, gate_w, up_w, down_w)


def rest_kernel(rows, layout, where_ref, *refs):
    pieces = refs[: len(layout)]
    (x_ref, cot_ref, oh_ref, og_ref, ou_ref, gate_ref, up_ref, down_ref) = refs[len(layout) : len(layout) + 8]
    (xa_ref, ca_ref, hid_ref, dg_ref, du_ref, mine_ref, theirs_ref, acc_ref) = refs[len(layout) + 8 :]
    step = pl.program_id(0)
    core, level = where_ref[1], where_ref[2]
    half = rows // 2
    chunks = xa_ref.shape[0] // rows - 1

    @pl.when(step == 0)
    def _():
        xa_ref[:rows, :] = x_ref[...]
        ca_ref[:rows, :] = cot_ref[...]
        for piece, (chunk, other_core, other_level) in zip(pieces, layout):
            count = piece.shape[1]
            start = rows * (chunk + 1) + (core ^ other_core) * half
            if count != half:
                start = start + ((level % 2) ^ other_level) * count
            start = pl.multiple_of(start, count)
            xa_ref[pl.ds(start, count), :] = piece[0]
            ca_ref[pl.ds(start, count), :] = piece[1]

    hid_ref[:rows, :] = oh_ref[...]
    dg_ref[:rows, :] = og_ref[...]
    du_ref[:rows, :] = ou_ref[...]
    hid, dg, du, grad = expert_math(
        xa_ref[rows:, :], ca_ref[rows:, :], gate_ref[...], up_ref[...], down_ref[...]
    )
    hid_ref[rows:, :], dg_ref[rows:, :], du_ref[rows:, :] = hid, dg, du

    @pl.when(step == 0)
    def _():
        acc_ref[...] = grad

    @pl.when(step != 0)
    def _():
        acc_ref[...] += grad

    @pl.when(step == pl.num_programs(0) - 1)
    def _():
        for chunk in range(chunks):
            start = pl.multiple_of(rows * chunk + core * half, half)
            mine_ref[chunk] = acc_ref[pl.ds(start, half), :]
            start = pl.multiple_of(rows * chunk + (1 - core) * half, half)
            theirs_ref[chunk] = acc_ref[pl.ds(start, half), :].astype(BF)


def rest_rows(place, pieces, layout, x, cot, own, gate_w, up_w, down_w, chunks):
    rows, width = x.shape
    hidden = gate_w.shape[1]
    tile = tile_of(hidden)
    total = rows * (chunks + 1)
    half = rows // 2

    def fixed(shape):
        return pl.BlockSpec(shape, lambda f: (0,) * len(shape))

    col = pl.BlockSpec((total, tile), lambda f: (0, f))
    own_col = pl.BlockSpec((rows, tile), lambda f: (0, f))
    return pl.pallas_call(
        functools.partial(rest_kernel, rows, layout),
        grid=(hidden // tile,),
        out_shape=[jax.ShapeDtypeStruct((total, width), BF)] * 2
        + [jax.ShapeDtypeStruct((total, hidden), BF)] * 3
        + [jax.ShapeDtypeStruct((chunks, half, width), F32), jax.ShapeDtypeStruct((chunks, half, width), BF)],
        in_specs=[SM]
        + [fixed(piece.shape) for piece in pieces]
        + [fixed(x.shape)] * 2
        + [own_col] * 3
        + [
            pl.BlockSpec((width, tile), lambda f: (0, f)),
            pl.BlockSpec((width, tile), lambda f: (0, f)),
            pl.BlockSpec((tile, width), lambda f: (f, 0)),
        ],
        out_specs=[fixed((total, width))] * 2
        + [col] * 3
        + [fixed((chunks, half, width))] * 2,
        scratch_shapes=[pltpu.VMEM((rows * chunks, width), F32)],
        compiler_params=pltpu.CompilerParams(vmem_limit_bytes=63 * 1024 * 1024),
        name="rest_rows",
    )(place, *pieces, x, cot, *own, gate_w, up_w, down_w)


def transposed_dot(a, b):
    return lax.dot_general(a, b, (((0,), (0,)), ((), ())), preferred_element_type=F32).astype(BF)


def pair_kernel(where_ref, mine_ref, theirs_ref, out_ref):
    out_ref[...] = (mine_ref[...] + theirs_ref[...].astype(F32)).astype(BF)


def split_kernel(groups, levels, where_ref, own_ref, part_ref, *refs):
    got = refs[: groups - 1]
    keep_ref = refs[groups - 1]
    sends = refs[groups:]
    half = part_ref.shape[0]
    share = half // levels
    core, level = where_ref[1], where_ref[2]
    for mask in range(levels):
        at = (level ^ mask) * share
        start = pl.multiple_of(core * half + at, share)
        here = pl.ds(pl.multiple_of(at, share), share)
        total = own_ref[pl.ds(start, share), :] + part_ref[here, :].astype(F32)
        for piece in got:
            total = total + piece[here, :].astype(F32)
        if mask == 0:
            keep_ref[...] = total
        else:
            sends[mask - 1][...] = total.astype(BF)


def join_kernel(where_ref, cot_ref, keep_ref, *refs):
    out_ref = refs[-1]
    share = keep_ref.shape[0]
    half = cot_ref.shape[0] // 2
    start = pl.multiple_of(where_ref[1] * half + where_ref[2] * share, share)
    total = cot_ref[pl.ds(start, share), :].astype(F32) + keep_ref[...]
    for piece in refs[:-1]:
        total = total + piece[...].astype(F32)
    out_ref[...] = total.astype(BF)


def on_device(
    moe_input, cotangent, route_expert, route_weight, w_gate, w_up, w_down, out_proj,
    saved_out, queries, keys, values, log_decay, span_state,
):
    rows, width = moe_input.shape
    half = rows // 2
    groups = lax.axis_size("sp")
    lanes = lax.axis_size("tp")
    if 4 * rows // groups < rows:
        return by_slots(
            moe_input, cotangent, route_expert, route_weight, w_gate, w_up, w_down, out_proj,
            saved_out, queries, keys, values, log_decay, span_state,
        )
    levels = lanes // 2
    share = half // levels
    mine = lax.axis_index("sp").astype(jnp.int32)
    lane = lax.axis_index("tp").astype(jnp.int32)
    core, level = lane % 2, lane // 2
    place = jnp.stack([mine, core, level])
    shared = [two_hops(mask) and levels > 1 for mask in range(groups)]
    gate_w, up_w, down_w = w_gate[0], w_up[0], w_down[0]

    *sends, own_cot = prepare(place, moe_input, cotangent, route_expert, route_weight, groups, shared)
    got = {}
    for mask in sorted(range(1, groups), key=lambda m: not shared[m]):
        got[mask] = swap(sends[mask - 1], "sp", mask)
    own = own_rows(place, moe_input, own_cot, gate_w, up_w, down_w)
    own_hid, own_dg, own_du, own_grad = own
    pieces, layout = [], []
    for mask in range(1, groups):
        arrived = [(got[mask], 0)]
        if shared[mask]:
            arrived.append((swap(got[mask], "tp", 2), 1))
        for piece, other_level in arrived:
            pieces += [piece, swap(piece, "tp", 1)]
            layout += [(mask - 1, 0, other_level), (mask - 1, 1, other_level)]
    all_x, all_cot, hid, dg, du, grad_mine, grad_theirs = rest_rows(
        place, pieces, tuple(layout), moe_input, own_cot, (own_hid, own_dg, own_du),
        gate_w, up_w, down_w, groups - 1,
    )
    own_theirs = lax.dynamic_slice_in_dim(own_grad, (1 - core) * half, half, 0).astype(BF)
    own_part = swap(own_theirs, "tp", 1)
    partner = swap(grad_theirs, "tp", 1)
    paired = pl.pallas_call(
        pair_kernel, out_shape=jax.ShapeDtypeStruct(grad_theirs.shape, BF),
        in_specs=[SM, VM, VM], out_specs=VM, name="pair",
    )(place, grad_mine, partner)
    back = [swap(paired[mask - 1], "sp", mask) for mask in range(1, groups)]
    grad_down = transposed_dot(hid, all_cot)
    grad_gate = transposed_dot(all_x, dg)
    grad_up = transposed_dot(all_x, du)
    small = jax.ShapeDtypeStruct((share, width), BF)
    keep, *outgoing = pl.pallas_call(
        functools.partial(split_kernel, groups, levels),
        out_shape=[jax.ShapeDtypeStruct((share, width), F32)] + [small] * (levels - 1),
        in_specs=[SM] + [VM] * (groups + 1), out_specs=[VM] * levels, name="split",
    )(place, own_grad, own_part, *back)
    incoming = [swap(piece, "tp", 2 * (mask + 1)) for mask, piece in enumerate(outgoing)]
    block = pl.pallas_call(
        join_kernel, out_shape=small, in_specs=[SM] + [VM] * (levels + 1), out_specs=VM, name="join",
    )(place, cotangent, keep, *incoming)
    stacked = jnp.stack([block] + [swap(block, "tp", 2 * mask) for mask in range(1, levels)])
    order = jnp.arange(levels, dtype=jnp.int32) ^ level
    upper_half = stacked[order].reshape(half, width)
    other_half = swap(upper_half, "tp", 1)
    first = jnp.where(core == 0, upper_half, other_half)
    second = jnp.where(core == 0, other_half, upper_half)
    grad_in = jnp.concatenate([first, second], axis=0)

    grad_mix = lax.dot_general(
        grad_in, out_proj, (((1,), (1,)), ((), ())), preferred_element_type=jnp.float32
    )
    slab = width // groups
    saved_all = [saved_out] + [swap(saved_out, "sp", mask) for mask in range(1, groups)]
    grad_cols = [lax.dynamic_slice_in_dim(grad_in, mine * slab, slab, 1)]
    for mask in range(1, groups):
        cols = lax.dynamic_slice_in_dim(grad_in, (mine ^ mask) * slab, slab, 1)
        grad_cols.append(swap(cols, "sp", mask))
    grad_proj = lax.dot_general(
        jnp.concatenate(grad_cols, 0), jnp.concatenate(saved_all, 0), (((0,), (0,)), ((), ())),
        preferred_element_type=F32,
    )
    pieces = gated_pieces(queries, keys, values, log_decay, grad_mix, DK, SPAN)
    g_local = pieces[9]
    last = pieces[5]
    begin = jnp.zeros(g_local.shape[1:], jnp.float32)
    device_start, local_end = lax.scan(backward_step, begin, (g_local, last), reverse=True)
    device_decay = jnp.exp(jnp.sum(last, axis=0))
    message = jnp.concatenate([device_start, jnp.broadcast_to(device_decay[..., None], device_decay.shape + (128,))], 1)
    state_after = begin
    for k in range(groups - 1, 0, -1):
        later = lax.ppermute(message, "sp", [(i, (i - k) % groups) for i in range(groups)])
        new = later[:, :DK] + later[:, DK:] * state_after
        state_after = jnp.where(mine + k < groups, new, state_after)
    running = jnp.cumsum(last, axis=0)
    beyond = running[-1][None] - running
    g_end = local_end + jnp.exp(beyond)[..., None] * state_after[None]
    grad_queries, grad_keys, grad_values, grad_decay = gated_finish(pieces, span_state, g_end, DK)
    return (
        grad_gate[None], grad_up[None], grad_down[None], grad_proj,
        grad_queries, grad_keys, grad_values, grad_decay,
    )


def solution(mesh):
    placed = (
        P("sp", None), P("sp", None), P("sp", None), P("sp", None),
        P("sp", None, "tp"), P("sp", None, "tp"), P("sp", "tp", None),
        P("tp", None), P("sp", "tp"), P("sp", "tp"), P("sp", "tp"),
        P("sp", "tp"), P("sp", "tp"), P("sp", "tp", None),
    )
    return jax.shard_map(
        on_device,
        mesh=mesh,
        in_specs=placed,
        out_specs=(
            P("sp", None, "tp"), P("sp", None, "tp"), P("sp", "tp", None),
            P("sp", "tp"), P("sp", "tp"), P("sp", "tp"), P("sp", "tp"), P("sp", "tp"),
        ),
        check_vma=False,
    )
```

```python
import functools

import jax
import jax.numpy as jnp
from jax import lax
from jax.experimental import pallas as pl
from jax.experimental.pallas import tpu as pltpu
from jax.sharding import PartitionSpec as P


DK = 64
SPAN = 64
HIGH = lax.Precision.HIGHEST
BF = jnp.bfloat16
F32 = jnp.float32


VM = pl.BlockSpec(memory_space=pltpu.VMEM)
HB = pl.BlockSpec(memory_space=pltpu.HBM)


def entering(shard, axis, combine, identity):
    length, mine = (lax.axis_size(axis), lax.axis_index(axis))
    everything = jax.tree.map(lambda part: lax.all_gather(part, axis), shard)
    start = jax.tree.map(
        lambda part, zero: jnp.broadcast_to(jnp.asarray(zero, part.dtype), part.shape),
        shard,
        identity,
    )

    def step(k, before):
        at = length - 1 - k
        reached = at > mine
        new = combine(before, jax.tree.map(lambda part: part[at], everything))
        return jax.tree.map(lambda a, b: jnp.where(reached, a, b), new, before)

    return lax.fori_loop(0, length, step, start)


def slot_places(experts, count):
    routes_flat = experts.reshape(-1)
    one_hot = (routes_flat[:, None] == jnp.arange(count, dtype=jnp.int32)[None, :]).astype(
        jnp.int32
    )
    earlier = jnp.cumsum(one_hot, axis=0) - one_hot
    return jnp.sum(earlier * one_hot, axis=1).reshape(experts.shape)


def expert_grads(inputs, routed, gate_weight, up_weight, down_weight):
    gate = jnp.dot(inputs, gate_weight, preferred_element_type=jnp.float32)
    upper = jnp.dot(inputs, up_weight, preferred_element_type=jnp.float32)
    sigmoid_gate = jax.nn.sigmoid(gate)
    active = gate * sigmoid_gate
    hidden = (active * upper).astype(jnp.bfloat16)
    d_hidden = lax.dot_general(
        routed, down_weight, (((1,), (1,)), ((), ())), preferred_element_type=jnp.float32
    )
    d_upper = (d_hidden * active).astype(jnp.bfloat16)
    d_gate = (d_hidden * upper * sigmoid_gate * (1.0 + gate * (1.0 - sigmoid_gate))).astype(
        jnp.bfloat16
    )
    grad_down = lax.dot_general(
        hidden, routed, (((0,), (0,)), ((), ())), preferred_element_type=jnp.float32
    ).astype(jnp.bfloat16)
    grad_gate = lax.dot_general(
        inputs, d_gate, (((0,), (0,)), ((), ())), preferred_element_type=jnp.float32
    ).astype(jnp.bfloat16)
    grad_up = lax.dot_general(
        inputs, d_upper, (((0,), (0,)), ((), ())), preferred_element_type=jnp.float32
    ).astype(jnp.bfloat16)
    return (d_gate, d_upper, grad_gate, grad_up, grad_down)


def input_grad(d_gate, d_upper, gate_weight, up_weight):
    first = lax.dot_general(
        d_gate, gate_weight, (((1,), (1,)), ((), ())), preferred_element_type=jnp.float32
    )
    second = lax.dot_general(
        d_upper, up_weight, (((1,), (1,)), ((), ())), preferred_element_type=jnp.float32
    )
    return first + second


def gated_pieces(queries, keys, values, log_decay, grad_mix, key_dim, span_len):
    value_dim = values.shape[1] * key_dim // queries.shape[1]
    heads = queries.shape[1] // key_dim
    spans = queries.shape[0] // span_len

    def blocks(array, width):
        return array.astype(jnp.float32).reshape(spans, span_len, heads, width)

    query_spans = blocks(queries, key_dim)
    key_spans = blocks(keys, key_dim)
    value_spans = blocks(values, value_dim)
    grad_spans = blocks(grad_mix, value_dim)
    cumulative = jnp.cumsum(blocks(log_decay, key_dim), axis=1)
    last = cumulative[:, -1]
    scale = key_dim ** (-0.5)
    query_decayed = query_spans * jnp.exp(cumulative)
    key_grown = key_spans * jnp.exp(-cumulative)
    key_to_end = key_spans * jnp.exp(last[:, None] - cumulative)
    g_local = scale * jnp.einsum("nthk,nthv->nhkv", query_decayed, grad_spans, precision=HIGH)
    return (
        query_spans,
        key_spans,
        value_spans,
        grad_spans,
        cumulative,
        last,
        query_decayed,
        key_grown,
        key_to_end,
        g_local,
    )


def backward_step(carry, inputs):
    local, decay = inputs
    return (local + jnp.exp(decay)[..., None] * carry, carry)


def gated_finish(pieces, span_state, g_end, key_dim):
    (
        query_spans,
        key_spans,
        value_spans,
        grad_spans,
        cumulative,
        last,
        query_decayed,
        key_grown,
        key_to_end,
        _,
    ) = pieces
    spans, span_len, heads, value_dim = value_spans.shape
    scale = key_dim ** (-0.5)
    token_locations = jnp.arange(span_len, dtype=jnp.int32)
    causal = (token_locations[:, None] >= token_locations[None, :]).astype(jnp.float32)
    scores = jnp.einsum("nthk,nshk->nhts", query_decayed, key_grown, precision=HIGH) * causal
    grad_dot = jnp.einsum("nthv,nshv->nhts", grad_spans, value_spans, precision=HIGH) * causal
    state = span_state.reshape(spans, heads, key_dim, value_dim)
    d_query = (
        scale
        * jnp.exp(cumulative)
        * (
            jnp.einsum("nhts,nshk->nthk", grad_dot, key_grown, precision=HIGH)
            + jnp.einsum("nthv,nhkv->nthk", grad_spans, state, precision=HIGH)
        )
    )
    d_key = scale * jnp.exp(-cumulative) * jnp.einsum(
        "nhts,nthk->nshk", grad_dot, query_decayed, precision=HIGH
    ) + jnp.exp(last[:, None] - cumulative) * jnp.einsum(
        "nshv,nhkv->nshk", value_spans, g_end, precision=HIGH
    )
    d_value = scale * jnp.einsum(
        "nhts,nthv->nshv", scores, grad_spans, precision=HIGH
    ) + jnp.einsum("nshk,nhkv->nshv", key_to_end, g_end, precision=HIGH)
    state_end = jnp.exp(last)[..., None] * state + jnp.einsum(
        "nshk,nshv->nhkv", key_to_end, value_spans, precision=HIGH
    )
    tail = jnp.sum(state_end * g_end, axis=-1)
    d_cumulative = query_spans * d_query - key_spans * d_key
    d_log = jnp.cumsum(d_cumulative[:, ::-1], axis=1)[:, ::-1] + tail[:, None]
    rows = spans * span_len
    return (
        d_query.reshape(rows, heads * key_dim).astype(jnp.bfloat16),
        d_key.reshape(rows, heads * key_dim).astype(jnp.bfloat16),
        d_value.reshape(rows, heads * value_dim).astype(jnp.bfloat16),
        d_log.reshape(rows, heads * key_dim),
    )


def carry_combine(earlier, later):
    return (later[0] * earlier[0], later[1] + later[0][..., None] * earlier[1])


def by_slots(
    moe_input,
    cotangent,
    route_expert,
    route_weight,
    w_gate,
    w_up,
    w_down,
    out_proj,
    saved_out,
    queries,
    keys,
    values,
    log_decay,
    span_state,
):
    tok_rows, width = moe_input.shape
    groups = lax.axis_size("sp")
    lanes = lax.axis_size("tp")
    capacity = 4 * tok_rows // groups
    target_locations = slot_places(route_expert, groups)
    rows_index = (target_locations * groups + route_expert).reshape(-1)
    owner = (
        jnp.full((capacity * groups,), 2 * tok_rows, jnp.int32)
        .at[rows_index]
        .set(jnp.arange(2 * tok_rows, dtype=jnp.int32))
    )
    weighted = (route_weight[:, :, None] * cotangent[:, None, :].astype(jnp.float32)).astype(
        jnp.bfloat16
    )
    weighted = weighted.reshape(2 * tok_rows, width)
    blank = jnp.zeros((1, width), jnp.bfloat16)
    send_in = jnp.concatenate([moe_input, blank], axis=0)[owner // 2].reshape(
        capacity, groups, width
    )
    send_cot = jnp.concatenate([weighted, blank], axis=0)[owner].reshape(capacity, groups, width)
    gate_weight = w_gate[0]
    up_weight = w_up[0]
    down_weight = w_down[0]
    share = capacity // lanes
    lane = lax.axis_index("tp")
    part_in = lax.dynamic_slice_in_dim(send_in, lane * share, share, 0)
    part_cot = lax.dynamic_slice_in_dim(send_cot, lane * share, share, 0)
    got_in, got_cot = (
        lax.all_to_all(part_in, "sp", split_axis=1, concat_axis=1, tiled=True),
        lax.all_to_all(part_cot, "sp", split_axis=1, concat_axis=1, tiled=True),
    )
    full_in, full_cot = (
        lax.all_gather(got_in, "tp", axis=0, tiled=True),
        lax.all_gather(got_cot, "tp", axis=0, tiled=True),
    )
    d_gate, d_upper, grad_gate, grad_up, grad_down = expert_grads(
        full_in.reshape(-1, width), full_cot.reshape(-1, width), gate_weight, up_weight, down_weight
    )
    mine = (
        lax.psum_scatter(
            input_grad(d_gate, d_upper, gate_weight, up_weight).astype(jnp.bfloat16),
            "tp",
            scatter_dimension=0,
            tiled=True,
        )
        .astype(jnp.float32)
        .reshape(share, groups, width)
    )
    returned = (
        lax.all_to_all(mine.astype(jnp.bfloat16), "sp", split_axis=1, concat_axis=1, tiled=True)
        .astype(mine.dtype)
        .reshape(-1, width)
    )
    local_index = rows_index - lane * share * groups
    inside = (local_index >= 0) & (local_index < share * groups)
    picked = jnp.where(inside[:, None], returned[jnp.clip(local_index, 0, share * groups - 1)], 0.0)
    routed = jnp.sum(picked.reshape(tok_rows, 2, width), axis=1)
    total = lax.psum(routed.astype(jnp.bfloat16), "tp").astype(jnp.float32)
    grad_in = (cotangent.astype(jnp.float32) + total).astype(jnp.bfloat16)
    grad_mix = lax.dot_general(
        grad_in, out_proj, (((1,), (1,)), ((), ())), preferred_element_type=jnp.float32
    )
    grad_proj = lax.psum_scatter(
        lax.dot_general(
            grad_in, saved_out, (((0,), (0,)), ((), ())), preferred_element_type=jnp.float32
        ).astype(jnp.bfloat16),
        "sp",
        scatter_dimension=0,
        tiled=True,
    ).astype(jnp.float32)
    pieces = gated_pieces(queries, keys, values, log_decay, grad_mix, DK, SPAN)
    g_local = pieces[9]
    last = pieces[5]
    begin = jnp.zeros(g_local.shape[1:], jnp.float32)
    device_start, local_end = lax.scan(backward_step, begin, (g_local, last), reverse=True)
    device_decay = jnp.exp(jnp.sum(last, axis=0))
    identity = (jnp.ones_like(device_decay), jnp.zeros_like(device_start))
    _, state_after = entering((device_decay, device_start), "sp", carry_combine, identity)
    running = jnp.cumsum(last, axis=0)
    beyond = running[-1][None] - running
    g_end = local_end + jnp.exp(beyond)[..., None] * state_after[None]
    grad_queries, grad_keys, grad_values, grad_decay = gated_finish(pieces, span_state, g_end, DK)
    return (
        grad_gate[None],
        grad_up[None],
        grad_down[None],
        grad_proj,
        grad_queries,
        grad_keys,
        grad_values,
        grad_decay,
    )


def nt(a, b):
    return lax.dot_general(a, b, (((1,), (1,)), ((), ())), preferred_element_type=F32)


def nn(a, b):
    return lax.dot_general(a, b, (((1,), (0,)), ((), ())), preferred_element_type=F32)


def swap(value, axis, mask):
    size = lax.axis_size(axis)
    return lax.ppermute(value, axis, [(i, i ^ mask) for i in range(size)])


def in_vmem(*values):
    return [pltpu.with_memory_space_constraint(value, pltpu.VMEM) for value in values]


def in_hbm(*values):
    return [pltpu.with_memory_space_constraint(value, pltpu.HBM) for value in values]


def spot():
    lane = lax.axis_index("tp")
    return lax.axis_index("sp"), lane % 2, lane // 2


def grant(mib):
    return pltpu.CompilerParams(vmem_limit_bytes=mib * 1024 * 1024)


def packed_weights(expert_ref, weight_ref):
    rows = expert_ref.shape[1]
    line = lax.broadcasted_iota(jnp.int32, (rows, rows), 0)
    table = jnp.zeros((rows, rows), F32)
    for choice in range(expert_ref.shape[0]):
        left = weight_ref[choice : choice + 1, :]
        named = line % 8 == expert_ref[choice : choice + 1, :]
        for part in range(3):
            piece = left.astype(BF).astype(F32)
            left = left - piece
            table = table + jnp.where(named & (line // 8 == part), piece, 0.0)
    return table.T


def column_of(table, expert):
    lane = lax.broadcasted_iota(jnp.int32, table.shape, 1)
    picked = (lane % 8 == expert) & (lane < 24)
    return jnp.sum(jnp.where(picked, table, 0.0), axis=1, keepdims=True)


def prep_kernel(x_ref, cot_ref, expert_ref, weight_ref, first_ref, second_ref, e_ref, w_ref, table_ref, sems):
    rows, width = x_ref.shape
    _, core, _ = spot()
    count = rows // 4
    copies = [
        pltpu.make_async_copy(expert_ref, e_ref, sems.at[0]),
        pltpu.make_async_copy(weight_ref, w_ref, sems.at[1]),
    ]
    for at, out in enumerate((first_ref, second_ref)):
        block = pl.ds(pl.multiple_of(core * 2 * count + at * count, count), count)
        for side, source in enumerate((x_ref, cot_ref)):
            target = out.at[:, pl.ds(side * width, width)]
            copies.append(pltpu.make_async_copy(source.at[block, :], target, sems.at[2 + 2 * at + side]))
    for copy in copies:
        copy.start()
    copies[0].wait()
    copies[1].wait()
    table_ref[...] = packed_weights(e_ref, w_ref)
    for at, out in enumerate((first_ref, second_ref)):
        block = pl.ds(pl.multiple_of(core * 2 * count + at * count, count), count)
        out[:, 2 * width :] = table_ref[block, :].astype(BF)
    for copy in copies[2:]:
        copy.wait()


def prepare(x, cot, expert, weight):
    rows, width = x.shape
    shape = jax.ShapeDtypeStruct((rows // 4, 2 * width + rows), BF)
    return pl.pallas_call(
        prep_kernel,
        out_shape=[shape] * 2,
        in_specs=[HB] * 4,
        out_specs=[VM] * 2,
        scratch_shapes=[
            pltpu.VMEM(expert.shape, jnp.int32),
            pltpu.VMEM(weight.shape, F32),
            pltpu.VMEM((rows, rows), F32),
            pltpu.SemaphoreType.DMA((6,)),
        ],
        compiler_params=grant(8),
        name="prep",
    )(*in_hbm(x, cot, expert, weight))


def start_all(sources, targets, sems):
    copies = [
        pltpu.make_async_copy(source, target, sems.at[at])
        for at, (source, target) in enumerate(zip(sources, targets))
    ]
    for copy in copies:
        copy.start()
    return copies


def wait_for(copies, at):
    if copies:
        copies[at].wait()


def through_expert(core, half, x_ref, mix_ref, weights, ready, hid_ref, dg_ref, du_ref, mine_ref, theirs_ref, acc_ref):
    gate_ref, up_ref, down_ref = weights
    wait_for(ready, 0)
    gate = nn(x_ref[...], gate_ref[...])
    sigmoid = 1.0 / (1.0 + jnp.exp(-gate))
    active = gate * sigmoid
    wait_for(ready, 1)
    upper = nn(x_ref[...], up_ref[...])
    hid_ref[...] = (active * upper).astype(BF)
    wait_for(ready, 2)
    d_hidden = nt(mix_ref[...], down_ref[...])
    du_ref[...] = (d_hidden * active).astype(BF)
    dg_ref[...] = (d_hidden * upper * sigmoid * (1.0 + gate * (1.0 - sigmoid))).astype(BF)
    acc_ref[...] = nt(dg_ref[...], gate_ref[...]) + nt(du_ref[...], up_ref[...])
    for chunk in range(mine_ref.shape[0]):
        start = pl.multiple_of((2 * chunk + core) * half, half)
        mine_ref[chunk] = acc_ref[pl.ds(start, half), :]
        start = pl.multiple_of((2 * chunk + 1 - core) * half, half)
        theirs_ref[chunk] = acc_ref[pl.ds(start, half), :].astype(BF)


def own_kernel(x_hbm, cot_hbm, expert_hbm, weight_hbm, gate_hbm, up_hbm, down_hbm, gate_ref, up_ref, down_ref, x_ref, mix_ref, *refs):
    outs, (acc_ref, cot_ref, e_ref, w_ref, sems) = refs[:5], refs[5:]
    mine, core, _ = spot()
    half = x_ref.shape[0] // 2
    copies = start_all(
        (expert_hbm, weight_hbm, x_hbm, cot_hbm, gate_hbm, up_hbm, down_hbm),
        (e_ref, w_ref, x_ref, cot_ref, gate_ref, up_ref, down_ref),
        sems,
    )
    for copy in copies[:4]:
        copy.wait()
    column = column_of(packed_weights(e_ref, w_ref), mine)
    mix_ref[...] = (column * cot_ref[...].astype(F32)).astype(BF)
    through_expert(core, half, x_ref, mix_ref, (gate_ref, up_ref, down_ref), copies[4:], *outs, acc_ref)


def expert_outs(rows, half, width, hidden):
    chunks = rows // (2 * half)
    return (
        [jax.ShapeDtypeStruct((rows, width), BF)] * 2
        + [jax.ShapeDtypeStruct((rows, hidden), BF)] * 3
        + [jax.ShapeDtypeStruct((chunks, half, width), F32), jax.ShapeDtypeStruct((chunks, half, width), BF)]
    )


def own_rows(x, cot, expert, weight, gate_w, up_w, down_w):
    rows, width = x.shape
    inputs = (x, cot, expert, weight, gate_w, up_w, down_w)
    return pl.pallas_call(
        own_kernel,
        out_shape=[pltpu.VMEM(one.shape, one.dtype) for one in inputs[4:]]
        + expert_outs(rows, rows // 2, width, gate_w.shape[1]),
        in_specs=[HB] * 7,
        out_specs=[VM] * 10,
        scratch_shapes=[pltpu.VMEM((rows, width), F32)]
        + [pltpu.VMEM(one.shape, one.dtype) for one in inputs[1:4]]
        + [pltpu.SemaphoreType.DMA((7,))],
        compiler_params=grant(10),
        name="own_rows",
    )(*in_hbm(*inputs))


def came_kernel(half, layout, *refs):
    pieces = refs[: len(layout)]
    weights = refs[len(layout) : len(layout) + 3]
    x_ref, mix_ref, *outs = refs[len(layout) + 3 : len(layout) + 10]
    (acc_ref,) = refs[len(layout) + 10 :]
    width = x_ref.shape[1]
    mine, core, _ = spot()
    for piece, (chunk, other, at) in zip(pieces, layout):
        count = piece.shape[0]
        start = (2 * chunk + (core ^ other)) * half + at * count
        block = pl.ds(pl.multiple_of(start, count), count)
        x_ref[block, :] = piece[:, :width]
        column = column_of(piece[:, 2 * width :].astype(F32), mine)
        mix_ref[block, :] = (column * piece[:, width : 2 * width].astype(F32)).astype(BF)
    through_expert(core, half, x_ref, mix_ref, weights, (), *outs, acc_ref)


def came_rows(chunks, half, width, pieces, layout, gate_w, up_w, down_w):
    rows = 2 * half * chunks
    held = (gate_w, up_w, down_w)
    return pl.pallas_call(
        functools.partial(came_kernel, half, layout),
        out_shape=expert_outs(rows, half, width, gate_w.shape[1]),
        in_specs=[VM] * len(pieces) + [VM] * 3,
        out_specs=[VM] * 7,
        scratch_shapes=[pltpu.VMEM((rows, width), F32)],
        compiler_params=grant(14),
    )(*pieces, *in_vmem(*held))


def collect_kernel(count, *refs):
    outs = refs[-count:]
    for kind, out in enumerate(outs):
        at = 0
        for part in refs[kind : len(refs) - count : count]:
            out[at : at + part.shape[0], :] = part[...]
            at += part.shape[0]


def collect(parts):
    count = len(parts[0])
    total = sum(part[0].shape[0] for part in parts)
    return pl.pallas_call(
        functools.partial(collect_kernel, count),
        out_shape=[jax.ShapeDtypeStruct((total, one.shape[1]), one.dtype) for one in parts[0]],
        in_specs=[VM] * (count * len(parts)),
        out_specs=[VM] * count,
        compiler_params=grant(20),
        name="collect",
    )(*[one for part in parts for one in part])


def transposed_dot(a, b):
    return lax.dot_general(a, b, (((0,), (0,)), ((), ())), preferred_element_type=F32).astype(BF)


def pair_kernel(mine_ref, theirs_ref, *outs):
    for chunk, out in enumerate(outs):
        out[...] = (mine_ref[chunk] + theirs_ref[chunk].astype(F32)).astype(BF)


def paired(mine, theirs):
    chunks, half, width = mine.shape
    return pl.pallas_call(
        pair_kernel, out_shape=[jax.ShapeDtypeStruct((half, width), BF)] * chunks,
        in_specs=[VM, VM], out_specs=[VM] * chunks, compiler_params=grant(6),
    )(mine, theirs)


def split_kernel(groups, levels, own_ref, part_ref, *refs):
    got = refs[: groups - 1]
    keep_ref = refs[groups - 1]
    sends = refs[groups:]
    half = part_ref.shape[0]
    share = half // levels
    _, _, level = spot()
    for mask in range(levels):
        here = pl.ds(pl.multiple_of((level ^ mask) * share, share), share)
        total = own_ref[here, :] + part_ref[here, :].astype(F32)
        for piece in got:
            total = total + piece[here, :].astype(F32)
        if mask == 0:
            keep_ref[...] = total
        else:
            sends[mask - 1][...] = total.astype(BF)


def join_kernel(cot_ref, keep_ref, *refs):
    out_ref = refs[-1]
    _, core, level = spot()
    share = keep_ref.shape[0]
    half = cot_ref.shape[0] // 2
    start = pl.multiple_of(core * half + level * share, share)
    total = cot_ref[pl.ds(start, share), :].astype(F32) + keep_ref[...]
    for piece in refs[:-1]:
        total = total + piece[...].astype(F32)
    out_ref[...] = total.astype(BF)


def cut_kernel(levels, groups, *refs):
    blocks, (half_ref, *cuts) = refs[:levels], refs[levels:]
    mine, _, level = spot()
    share = blocks[0].shape[0]
    for mask, block in enumerate(blocks):
        half_ref[pl.ds(pl.multiple_of((level ^ mask) * share, share), share), :] = block[...]
    slab = half_ref.shape[1] // groups
    for mask, cut in enumerate(cuts):
        cut[...] = half_ref[:, pl.ds(pl.multiple_of((mine ^ mask) * slab, slab), slab)]


def exact(a, b, contract):
    return lax.dot_general(
        a, b, ((contract[:1], contract[1:]), ((), ())), precision=HIGH, preferred_element_type=F32
    )


def grown_kernel(q_ref, k_ref, decay_ref, state_ref, grown_ref, last_ref, scores_ref, turned_ref):
    spans, heads = scores_ref.shape[:2]
    at = lax.broadcasted_iota(jnp.int32, (SPAN, SPAN), 0)
    to = lax.broadcasted_iota(jnp.int32, (SPAN, SPAN), 1)
    causal = (at >= to).astype(F32)
    channel = lax.broadcasted_iota(jnp.int32, (1, q_ref.shape[1]), 1) // DK
    scale = DK ** (-0.5)
    for span in range(spans):
        here = slice(span * SPAN, (span + 1) * SPAN)
        cumulative = exact(causal, decay_ref[here, :], (1, 0))
        last = cumulative[SPAN - 1 :, :]
        last_ref[span] = jnp.broadcast_to(last, last_ref.shape[1:])
        up, down = jnp.exp(cumulative), jnp.exp(-cumulative)
        ending = jnp.exp(last - cumulative)
        keys = k_ref[here, :].astype(F32)
        grown, shrunk = q_ref[here, :].astype(F32) * up, keys * down
        for kind, value in enumerate((grown, shrunk, keys * ending, scale * up, scale * down, ending)):
            grown_ref[kind, here, :] = value
        for head in range(heads):
            own = jnp.where(channel == head, grown, 0.0)
            scores_ref[span, head] = scale * exact(own, shrunk, (1, 1)) * causal
        turned_ref[span] = state_ref[span].T


def mix_kernel(first_ref, second_ref, proj_ref, grown_ref, last_ref, mix_ref, local_ref, message_ref, both_ref):
    _, core, _ = spot()
    half = first_ref.shape[0]
    both_ref[pl.ds(pl.multiple_of(core * half, half), half), :] = first_ref[...]
    both_ref[pl.ds(pl.multiple_of((1 - core) * half, half), half), :] = second_ref[...]
    mix_ref[...] = nt(both_ref[...], proj_ref[...])
    spans, value_dim = local_ref.shape[0], local_ref.shape[1]
    channel = lax.broadcasted_iota(jnp.int32, (1, local_ref.shape[2]), 1) // DK
    heads = local_ref.shape[2] // DK
    carry = jnp.zeros(local_ref.shape[1:], F32)
    total = jnp.zeros((8, local_ref.shape[2]), F32)
    for span in reversed(range(spans)):
        here = slice(span * SPAN, (span + 1) * SPAN)
        query = grown_ref[0, here, :] * (DK ** (-0.5))
        grads = jnp.concatenate(
            [mix_ref[here, head * value_dim : (head + 1) * value_dim] for head in range(heads)], 0
        )
        queries = jnp.concatenate([jnp.where(channel == head, query, 0.0) for head in range(heads)], 0)
        local = exact(grads, queries, (0, 0))
        local_ref[span] = local
        carry = local + jnp.exp(last_ref[span][:1, :]) * carry
        total = total + last_ref[span]
    message_ref[:value_dim, :] = carry
    message_ref[value_dim:, :] = jnp.exp(total)


def within_kernel(mix_ref, v_ref, grown_ref, scores_ref, state_ref, dq_ref, dk_ref, dv_ref):
    spans, heads = scores_ref.shape[:2]
    value_dim = v_ref.shape[1] // heads
    channel = lax.broadcasted_iota(jnp.int32, (1, heads * DK), 1) // DK
    line = lax.broadcasted_iota(jnp.int32, (heads * DK, 1), 0) // DK
    at = lax.broadcasted_iota(jnp.int32, (SPAN, SPAN), 0)
    to = lax.broadcasted_iota(jnp.int32, (SPAN, SPAN), 1)
    causal = (at >= to).astype(F32)
    for span in range(spans):
        here = slice(span * SPAN, (span + 1) * SPAN)
        query, key = grown_ref[0, here, :], grown_ref[1, here, :]
        dots = []
        for head in range(heads):
            wide = slice(head * value_dim, (head + 1) * value_dim)
            grads = mix_ref[here, wide]
            dots.append(exact(grads, v_ref[here, wide].astype(F32), (1, 1)) * causal)
            dv_ref[here, wide] = exact(scores_ref[span, head], grads, (0, 0))
        keys = jnp.concatenate([jnp.where(channel == head, key, 0.0) for head in range(heads)], 0)
        queries = jnp.concatenate([jnp.where(channel == head, query, 0.0) for head in range(heads)], 0)
        state = jnp.concatenate([jnp.where(line == head, state_ref[span], 0.0) for head in range(heads)], 1)
        dq = exact(jnp.concatenate(dots, 1), keys, (1, 0)) + exact(mix_ref[here, :], state, (1, 1))
        dq_ref[here, :] = grown_ref[3, here, :] * dq
        dk_ref[here, :] = grown_ref[4, here, :] * exact(jnp.concatenate(dots, 0), queries, (0, 0))


def final_kernel(groups, *refs):
    messages = refs[: groups - 1]
    (q_ref, k_ref, v_ref, grown_ref, last_ref, turned_ref, local_ref, dq_ref, dk_ref, dv_ref) = refs[
        groups - 1 : groups + 9
    ]
    q_out, k_out, v_out, decay_out = refs[groups + 9 :]
    mine, _, _ = spot()
    spans, value_dim, channels = local_ref.shape
    heads = channels // DK
    channel = lax.broadcasted_iota(jnp.int32, (1, channels), 1) // DK
    at = lax.broadcasted_iota(jnp.int32, (SPAN, SPAN), 0)
    to = lax.broadcasted_iota(jnp.int32, (SPAN, SPAN), 1)
    onward = (at <= to).astype(F32)
    ending = jnp.zeros((value_dim, channels), F32)
    for ahead in reversed(range(1, groups)):
        message = messages[ahead - 1]
        passed = message[:value_dim, :] + message[value_dim : value_dim + 1, :] * ending
        ending = jnp.where(mine + ahead < groups, passed, ending)
    for span in reversed(range(spans)):
        here = slice(span * SPAN, (span + 1) * SPAN)
        values = v_ref[here, :].astype(F32)
        last = jnp.exp(last_ref[span][:1, :])
        key_end = grown_ref[2, here, :]
        ends = jnp.concatenate([jnp.where(channel == head, ending, 0.0) for head in range(heads)], 0)
        through = exact(values, ends, (1, 0))
        dq = dq_ref[here, :]
        dk = dk_ref[here, :] + grown_ref[5, here, :] * through
        for head in range(heads):
            wide = slice(head * value_dim, (head + 1) * value_dim)
            own = jnp.where(channel == head, key_end, 0.0)
            v_out[here, wide] = (dv_ref[here, wide] + exact(own, ending, (1, 1))).astype(BF)
        tail = last * jnp.sum(turned_ref[span] * ending, axis=0, keepdims=True)
        tail = tail + jnp.sum(key_end * through, axis=0, keepdims=True)
        change = q_ref[here, :].astype(F32) * dq - k_ref[here, :].astype(F32) * dk
        decay_out[here, :] = exact(onward, change, (1, 0)) + tail
        q_out[here, :] = dq.astype(BF)
        k_out[here, :] = dk.astype(BF)
        ending = local_ref[span] + last * ending


def proj_kernel(groups, *refs):
    out_ref, left_ref, right_ref = refs[-3:]
    _, core, _ = spot()
    half = refs[0].shape[0]
    rows = 2 * half
    for group in range(groups):
        own, other, saved = refs[3 * group : 3 * group + 3]
        left_ref[pl.ds(pl.multiple_of(group * rows + core * half, half), half), :] = own[...]
        left_ref[pl.ds(pl.multiple_of(group * rows + (1 - core) * half, half), half), :] = other[...]
        right_ref[group * rows : (group + 1) * rows, :] = saved[...]
    out_ref[...] = lax.dot_general(
        left_ref[...], right_ref[...], (((0,), (0,)), ((), ())), preferred_element_type=F32
    )


def call(kernel, outs, args, mib, scratch=()):
    return pl.pallas_call(
        kernel, out_shape=outs, in_specs=[VM] * len(args), out_specs=[VM] * len(outs),
        scratch_shapes=scratch, compiler_params=grant(mib),
    )(*args)


def like(*shape, dtype=F32):
    return jax.ShapeDtypeStruct(shape, dtype)


def whole_rows(mesh):
    return mesh.shape["sp"] == 4 and mesh.shape["tp"] % 2 == 0


def by_rows(*args):
    return rows_on_device(*args)


def rows_on_device(
    moe_input, cotangent, route_expert, route_weight, w_gate, w_up, w_down, out_proj,
    saved_out, queries, keys, values, log_decay, span_state,
):
    rows, width = moe_input.shape
    half = rows // 2
    groups = lax.axis_size("sp")
    lanes = lax.axis_size("tp")
    levels = lanes // 2
    share = half // levels
    mine = lax.axis_index("sp").astype(jnp.int32)
    lane = lax.axis_index("tp").astype(jnp.int32)
    gate_w, up_w, down_w = w_gate[0], w_up[0], w_down[0]
    expert_t, weight_t = route_expert.T, route_weight.T

    first, second = prepare(moe_input, cotangent, expert_t, weight_t)
    x_first = swap(first, "sp", 1)
    y_second = swap(second, "sp", 2)
    x_second = swap(second, "sp", 1)
    y_first = swap(first, "sp", 2)
    x_first, y_second, expert_own = lax.optimization_barrier((x_first, y_second, expert_t))
    d_first = swap(x_first, "sp", 2)
    d_second = swap(y_second, "sp", 1)
    gate_w, up_w, down_w, own_x, own_cot, own_hid, own_dg, own_du, own_mine, own_theirs = own_rows(
        moe_input, cotangent, expert_own, weight_t, gate_w, up_w, down_w
    )
    x_second, y_first, own_theirs = lax.optimization_barrier((x_second, y_first, own_theirs))
    own_part = swap(own_theirs, "tp", 1)
    near, far = [x_first, x_second, y_first, y_second], [d_first, d_second]
    near_layout = [(chunk, other, at) for other in range(2) for chunk in range(2) for at in range(2)]
    far_layout = [(0, other, at) for other in range(2) for at in range(2)]
    near += [swap(piece, "tp", 1) for piece in near]
    near_x, near_cot, near_hid, near_dg, near_du, near_mine, near_theirs = came_rows(
        2, half, width, near, tuple(near_layout), gate_w, up_w, down_w
    )
    near_back = paired(near_mine, swap(near_theirs, "tp", 1))
    far += [swap(piece, "tp", 1) for piece in far]
    *far, near_one, near_two = lax.optimization_barrier((*far, *near_back))
    back = [swap(near_one, "sp", 1)]
    back.append(swap(near_two, "sp", 2))
    far_x, far_cot, far_hid, far_dg, far_du, far_mine, far_theirs = came_rows(
        1, half, width, far, tuple(far_layout), gate_w, up_w, down_w
    )
    (far_back,) = paired(far_mine, swap(far_theirs, "tp", 1))
    back.append(swap(far_back, "sp", 3))
    all_x, all_cot, hid, dg, du = collect(
        [
            [own_x, own_cot, own_hid, own_dg, own_du],
            [near_x, near_cot, near_hid, near_dg, near_du],
            [far_x, far_cot, far_hid, far_dg, far_du],
        ]
    )
    grad_down = transposed_dot(hid, all_cot)
    *back, grad_down = lax.optimization_barrier((*back, grad_down))
    grad_gate = transposed_dot(all_x, dg)
    small = jax.ShapeDtypeStruct((share, width), BF)
    keep, *outgoing = pl.pallas_call(
        functools.partial(split_kernel, groups, levels),
        out_shape=[jax.ShapeDtypeStruct((share, width), F32)] + [small] * (levels - 1),
        in_specs=[VM] * (groups + 1), out_specs=[VM] * levels, name="split", compiler_params=grant(6),
    )(own_mine[0], own_part[0], *back)
    incoming = []
    for mask, piece in enumerate(outgoing):
        incoming.append(swap(piece, "tp", 2 * (mask + 1)))
    grad_up = transposed_dot(all_x, du)
    keep, saved_send = lax.optimization_barrier((keep, saved_out))
    saved_all = [saved_out]
    for mask in range(1, groups):
        saved_all.append(swap(saved_send, "sp", mask))
    *incoming, grad_gate = lax.optimization_barrier((*incoming, grad_gate))
    (block,) = call(join_kernel, [small], (cotangent, keep, *incoming), 6)
    blocks = [block]
    for mask in range(1, levels):
        blocks.append(swap(block, "tp", 2 * mask))
    *blocks, grad_up = lax.optimization_barrier((*blocks, grad_up))
    slab = width // groups
    this_half, *cuts = call(
        functools.partial(cut_kernel, levels, groups),
        [like(half, width, dtype=BF)] + [like(half, slab, dtype=BF)] * groups, blocks, 6,
    )
    other_half = swap(this_half, "tp", 1)
    got_cuts = [cuts[0]]
    for mask in range(1, groups):
        got_cuts.append(swap(cuts[mask], "sp", mask))

    channels, value_dim = queries.shape[1], values.shape[1] * DK // queries.shape[1]
    spans, heads = rows // SPAN, channels // DK
    grown, last, scores, turned = call(
        grown_kernel,
        [like(6, rows, channels), like(spans, 8, channels), like(spans, heads, SPAN, SPAN),
         like(spans, value_dim, channels)],
        (queries, keys, log_decay, span_state), 6,
    )
    mix, local, message = call(
        mix_kernel,
        [like(rows, heads * value_dim), like(spans, value_dim, channels), like(value_dim + 8, channels)],
        (this_half, other_half, out_proj, grown, last), 8,
        [pltpu.VMEM((rows, width), BF)],
    )
    messages = []
    for ahead in range(1, groups):
        messages.append(lax.ppermute(message, "sp", [(i, i - ahead) for i in range(ahead, groups)]))
    dq, dk, dv = call(
        within_kernel, [like(rows, channels)] * 2 + [like(rows, heads * value_dim)],
        (mix, values, grown, scores, span_state), 6,
    )
    parts = []
    for mask in range(groups):
        parts += [got_cuts[mask], swap(got_cuts[mask], "tp", 1), saved_all[mask]]
    (grad_proj,) = call(
        functools.partial(proj_kernel, groups), [like(slab, saved_out.shape[1])], parts, 8,
        [pltpu.VMEM((groups * rows, slab), BF), pltpu.VMEM((groups * rows, saved_out.shape[1]), BF)],
    )
    grad_queries, grad_keys, grad_values, grad_decay = call(
        functools.partial(final_kernel, groups),
        [like(rows, channels, dtype=BF)] * 2 + [like(rows, heads * value_dim, dtype=BF), like(rows, channels)],
        (*messages, queries, keys, values, grown, last, turned, local, dq, dk, dv), 8,
    )
    return (
        grad_gate[None], grad_up[None], grad_down[None], grad_proj,
        grad_queries, grad_keys, grad_values, grad_decay,
    )


def solution(mesh):
    placed = (
        P("sp", None), P("sp", None), P("sp", None), P("sp", None),
        P("sp", None, "tp"), P("sp", None, "tp"), P("sp", "tp", None),
        P("tp", None), P("sp", "tp"), P("sp", "tp"), P("sp", "tp"),
        P("sp", "tp"), P("sp", "tp"), P("sp", "tp", None),
    )
    return jax.shard_map(
        by_rows if whole_rows(mesh) else by_slots,
        mesh=mesh,
        in_specs=placed,
        out_specs=(
            P("sp", None, "tp"), P("sp", None, "tp"), P("sp", "tp", None),
            P("sp", "tp"), P("sp", "tp"), P("sp", "tp"), P("sp", "tp"), P("sp", "tp"),
        ),
        check_vma=False,
    )
```

```python
import functools

import jax
import jax.numpy as jnp
from jax import lax
from jax.experimental import pallas as pl
from jax.experimental.pallas import tpu as pltpu
from jax.sharding import PartitionSpec as P


DK = 64
SPAN = 64
HIGH = lax.Precision.HIGHEST
BF = jnp.bfloat16
F32 = jnp.float32


VM = pl.BlockSpec(memory_space=pltpu.VMEM)
HB = pl.BlockSpec(memory_space=pltpu.HBM)


def entering(shard, axis, combine, identity):
    length, mine = (lax.axis_size(axis), lax.axis_index(axis))
    everything = jax.tree.map(lambda part: lax.all_gather(part, axis), shard)
    start = jax.tree.map(
        lambda part, zero: jnp.broadcast_to(jnp.asarray(zero, part.dtype), part.shape),
        shard,
        identity,
    )

    def step(k, before):
        at = length - 1 - k
        reached = at > mine
        new = combine(before, jax.tree.map(lambda part: part[at], everything))
        return jax.tree.map(lambda a, b: jnp.where(reached, a, b), new, before)

    return lax.fori_loop(0, length, step, start)


def slot_places(experts, count):
    routes_flat = experts.reshape(-1)
    one_hot = (routes_flat[:, None] == jnp.arange(count, dtype=jnp.int32)[None, :]).astype(
        jnp.int32
    )
    earlier = jnp.cumsum(one_hot, axis=0) - one_hot
    return jnp.sum(earlier * one_hot, axis=1).reshape(experts.shape)


def expert_grads(inputs, routed, gate_weight, up_weight, down_weight):
    gate = jnp.dot(inputs, gate_weight, preferred_element_type=jnp.float32)
    upper = jnp.dot(inputs, up_weight, preferred_element_type=jnp.float32)
    sigmoid_gate = jax.nn.sigmoid(gate)
    active = gate * sigmoid_gate
    hidden = (active * upper).astype(jnp.bfloat16)
    d_hidden = lax.dot_general(
        routed, down_weight, (((1,), (1,)), ((), ())), preferred_element_type=jnp.float32
    )
    d_upper = (d_hidden * active).astype(jnp.bfloat16)
    d_gate = (d_hidden * upper * sigmoid_gate * (1.0 + gate * (1.0 - sigmoid_gate))).astype(
        jnp.bfloat16
    )
    grad_down = lax.dot_general(
        hidden, routed, (((0,), (0,)), ((), ())), preferred_element_type=jnp.float32
    ).astype(jnp.bfloat16)
    grad_gate = lax.dot_general(
        inputs, d_gate, (((0,), (0,)), ((), ())), preferred_element_type=jnp.float32
    ).astype(jnp.bfloat16)
    grad_up = lax.dot_general(
        inputs, d_upper, (((0,), (0,)), ((), ())), preferred_element_type=jnp.float32
    ).astype(jnp.bfloat16)
    return (d_gate, d_upper, grad_gate, grad_up, grad_down)


def input_grad(d_gate, d_upper, gate_weight, up_weight):
    first = lax.dot_general(
        d_gate, gate_weight, (((1,), (1,)), ((), ())), preferred_element_type=jnp.float32
    )
    second = lax.dot_general(
        d_upper, up_weight, (((1,), (1,)), ((), ())), preferred_element_type=jnp.float32
    )
    return first + second


def gated_pieces(queries, keys, values, log_decay, grad_mix, key_dim, span_len):
    value_dim = values.shape[1] * key_dim // queries.shape[1]
    heads = queries.shape[1] // key_dim
    spans = queries.shape[0] // span_len

    def blocks(array, width):
        return array.astype(jnp.float32).reshape(spans, span_len, heads, width)

    query_spans = blocks(queries, key_dim)
    key_spans = blocks(keys, key_dim)
    value_spans = blocks(values, value_dim)
    grad_spans = blocks(grad_mix, value_dim)
    cumulative = jnp.cumsum(blocks(log_decay, key_dim), axis=1)
    last = cumulative[:, -1]
    scale = key_dim ** (-0.5)
    query_decayed = query_spans * jnp.exp(cumulative)
    key_grown = key_spans * jnp.exp(-cumulative)
    key_to_end = key_spans * jnp.exp(last[:, None] - cumulative)
    g_local = scale * jnp.einsum("nthk,nthv->nhkv", query_decayed, grad_spans, precision=HIGH)
    return (
        query_spans,
        key_spans,
        value_spans,
        grad_spans,
        cumulative,
        last,
        query_decayed,
        key_grown,
        key_to_end,
        g_local,
    )


def backward_step(carry, inputs):
    local, decay = inputs
    return (local + jnp.exp(decay)[..., None] * carry, carry)


def gated_finish(pieces, span_state, g_end, key_dim):
    (
        query_spans,
        key_spans,
        value_spans,
        grad_spans,
        cumulative,
        last,
        query_decayed,
        key_grown,
        key_to_end,
        _,
    ) = pieces
    spans, span_len, heads, value_dim = value_spans.shape
    scale = key_dim ** (-0.5)
    token_locations = jnp.arange(span_len, dtype=jnp.int32)
    causal = (token_locations[:, None] >= token_locations[None, :]).astype(jnp.float32)
    scores = jnp.einsum("nthk,nshk->nhts", query_decayed, key_grown, precision=HIGH) * causal
    grad_dot = jnp.einsum("nthv,nshv->nhts", grad_spans, value_spans, precision=HIGH) * causal
    state = span_state.reshape(spans, heads, key_dim, value_dim)
    d_query = (
        scale
        * jnp.exp(cumulative)
        * (
            jnp.einsum("nhts,nshk->nthk", grad_dot, key_grown, precision=HIGH)
            + jnp.einsum("nthv,nhkv->nthk", grad_spans, state, precision=HIGH)
        )
    )
    d_key = scale * jnp.exp(-cumulative) * jnp.einsum(
        "nhts,nthk->nshk", grad_dot, query_decayed, precision=HIGH
    ) + jnp.exp(last[:, None] - cumulative) * jnp.einsum(
        "nshv,nhkv->nshk", value_spans, g_end, precision=HIGH
    )
    d_value = scale * jnp.einsum(
        "nhts,nthv->nshv", scores, grad_spans, precision=HIGH
    ) + jnp.einsum("nshk,nhkv->nshv", key_to_end, g_end, precision=HIGH)
    state_end = jnp.exp(last)[..., None] * state + jnp.einsum(
        "nshk,nshv->nhkv", key_to_end, value_spans, precision=HIGH
    )
    tail = jnp.sum(state_end * g_end, axis=-1)
    d_cumulative = query_spans * d_query - key_spans * d_key
    d_log = jnp.cumsum(d_cumulative[:, ::-1], axis=1)[:, ::-1] + tail[:, None]
    rows = spans * span_len
    return (
        d_query.reshape(rows, heads * key_dim).astype(jnp.bfloat16),
        d_key.reshape(rows, heads * key_dim).astype(jnp.bfloat16),
        d_value.reshape(rows, heads * value_dim).astype(jnp.bfloat16),
        d_log.reshape(rows, heads * key_dim),
    )


def carry_combine(earlier, later):
    return (later[0] * earlier[0], later[1] + later[0][..., None] * earlier[1])


def by_slots(
    moe_input,
    cotangent,
    route_expert,
    route_weight,
    w_gate,
    w_up,
    w_down,
    out_proj,
    saved_out,
    queries,
    keys,
    values,
    log_decay,
    span_state,
):
    tok_rows, width = moe_input.shape
    groups = lax.axis_size("sp")
    lanes = lax.axis_size("tp")
    capacity = 4 * tok_rows // groups
    target_locations = slot_places(route_expert, groups)
    rows_index = (target_locations * groups + route_expert).reshape(-1)
    owner = (
        jnp.full((capacity * groups,), 2 * tok_rows, jnp.int32)
        .at[rows_index]
        .set(jnp.arange(2 * tok_rows, dtype=jnp.int32))
    )
    weighted = (route_weight[:, :, None] * cotangent[:, None, :].astype(jnp.float32)).astype(
        jnp.bfloat16
    )
    weighted = weighted.reshape(2 * tok_rows, width)
    blank = jnp.zeros((1, width), jnp.bfloat16)
    send_in = jnp.concatenate([moe_input, blank], axis=0)[owner // 2].reshape(
        capacity, groups, width
    )
    send_cot = jnp.concatenate([weighted, blank], axis=0)[owner].reshape(capacity, groups, width)
    gate_weight = w_gate[0]
    up_weight = w_up[0]
    down_weight = w_down[0]
    share = capacity // lanes
    lane = lax.axis_index("tp")
    part_in = lax.dynamic_slice_in_dim(send_in, lane * share, share, 0)
    part_cot = lax.dynamic_slice_in_dim(send_cot, lane * share, share, 0)
    got_in, got_cot = (
        lax.all_to_all(part_in, "sp", split_axis=1, concat_axis=1, tiled=True),
        lax.all_to_all(part_cot, "sp", split_axis=1, concat_axis=1, tiled=True),
    )
    full_in, full_cot = (
        lax.all_gather(got_in, "tp", axis=0, tiled=True),
        lax.all_gather(got_cot, "tp", axis=0, tiled=True),
    )
    d_gate, d_upper, grad_gate, grad_up, grad_down = expert_grads(
        full_in.reshape(-1, width), full_cot.reshape(-1, width), gate_weight, up_weight, down_weight
    )
    mine = (
        lax.psum_scatter(
            input_grad(d_gate, d_upper, gate_weight, up_weight).astype(jnp.bfloat16),
            "tp",
            scatter_dimension=0,
            tiled=True,
        )
        .astype(jnp.float32)
        .reshape(share, groups, width)
    )
    returned = (
        lax.all_to_all(mine.astype(jnp.bfloat16), "sp", split_axis=1, concat_axis=1, tiled=True)
        .astype(mine.dtype)
        .reshape(-1, width)
    )
    local_index = rows_index - lane * share * groups
    inside = (local_index >= 0) & (local_index < share * groups)
    picked = jnp.where(inside[:, None], returned[jnp.clip(local_index, 0, share * groups - 1)], 0.0)
    routed = jnp.sum(picked.reshape(tok_rows, 2, width), axis=1)
    total = lax.psum(routed.astype(jnp.bfloat16), "tp").astype(jnp.float32)
    grad_in = (cotangent.astype(jnp.float32) + total).astype(jnp.bfloat16)
    grad_mix = lax.dot_general(
        grad_in, out_proj, (((1,), (1,)), ((), ())), preferred_element_type=jnp.float32
    )
    grad_proj = lax.psum_scatter(
        lax.dot_general(
            grad_in, saved_out, (((0,), (0,)), ((), ())), preferred_element_type=jnp.float32
        ).astype(jnp.bfloat16),
        "sp",
        scatter_dimension=0,
        tiled=True,
    ).astype(jnp.float32)
    pieces = gated_pieces(queries, keys, values, log_decay, grad_mix, DK, SPAN)
    g_local = pieces[9]
    last = pieces[5]
    begin = jnp.zeros(g_local.shape[1:], jnp.float32)
    device_start, local_end = lax.scan(backward_step, begin, (g_local, last), reverse=True)
    device_decay = jnp.exp(jnp.sum(last, axis=0))
    identity = (jnp.ones_like(device_decay), jnp.zeros_like(device_start))
    _, state_after = entering((device_decay, device_start), "sp", carry_combine, identity)
    running = jnp.cumsum(last, axis=0)
    beyond = running[-1][None] - running
    g_end = local_end + jnp.exp(beyond)[..., None] * state_after[None]
    grad_queries, grad_keys, grad_values, grad_decay = gated_finish(pieces, span_state, g_end, DK)
    return (
        grad_gate[None],
        grad_up[None],
        grad_down[None],
        grad_proj,
        grad_queries,
        grad_keys,
        grad_values,
        grad_decay,
    )


def nt(a, b):
    return lax.dot_general(a, b, (((1,), (1,)), ((), ())), preferred_element_type=F32)


def nn(a, b):
    return lax.dot_general(a, b, (((1,), (0,)), ((), ())), preferred_element_type=F32)


def swap(value, axis, mask):
    size = lax.axis_size(axis)
    return lax.ppermute(value, axis, [(i, i ^ mask) for i in range(size)])


def in_vmem(*values):
    return [pltpu.with_memory_space_constraint(value, pltpu.VMEM) for value in values]


def in_hbm(*values):
    return [pltpu.with_memory_space_constraint(value, pltpu.HBM) for value in values]


def spot():
    lane = lax.axis_index("tp")
    return lax.axis_index("sp"), lane % 2, lane // 2


def grant(mib):
    return pltpu.CompilerParams(vmem_limit_bytes=mib * 1024 * 1024)


def packed_weights(expert_ref, weight_ref):
    rows = expert_ref.shape[1]
    line = lax.broadcasted_iota(jnp.int32, (rows, rows), 0)
    table = jnp.zeros((rows, rows), F32)
    for choice in range(expert_ref.shape[0]):
        left = weight_ref[choice : choice + 1, :]
        named = line % 8 == expert_ref[choice : choice + 1, :]
        for part in range(3):
            piece = left.astype(BF).astype(F32)
            left = left - piece
            table = table + jnp.where(named & (line // 8 == part), piece, 0.0)
    return table.T


def column_of(table, expert):
    lane = lax.broadcasted_iota(jnp.int32, table.shape, 1)
    picked = (lane % 8 == expert) & (lane < 24)
    return jnp.sum(jnp.where(picked, table, 0.0), axis=1, keepdims=True)


def prep_kernel(x_ref, cot_ref, expert_ref, weight_ref, first_ref, second_ref, e_ref, w_ref, table_ref, sems):
    rows, width = x_ref.shape
    _, core, _ = spot()
    count = rows // 4
    copies = [
        pltpu.make_async_copy(expert_ref, e_ref, sems.at[0]),
        pltpu.make_async_copy(weight_ref, w_ref, sems.at[1]),
    ]
    for at, out in enumerate((first_ref, second_ref)):
        block = pl.ds(pl.multiple_of(core * 2 * count + at * count, count), count)
        for side, source in enumerate((x_ref, cot_ref)):
            target = out.at[:, pl.ds(side * width, width)]
            copies.append(pltpu.make_async_copy(source.at[block, :], target, sems.at[2 + 2 * at + side]))
    for copy in copies:
        copy.start()
    copies[0].wait()
    copies[1].wait()
    table_ref[...] = packed_weights(e_ref, w_ref)
    for at, out in enumerate((first_ref, second_ref)):
        block = pl.ds(pl.multiple_of(core * 2 * count + at * count, count), count)
        out[:, 2 * width :] = table_ref[block, :].astype(BF)
    for copy in copies[2:]:
        copy.wait()


def prepare(x, cot, expert, weight):
    rows, width = x.shape
    shape = jax.ShapeDtypeStruct((rows // 4, 2 * width + rows), BF)
    return pl.pallas_call(
        prep_kernel,
        out_shape=[shape] * 2,
        in_specs=[HB] * 4,
        out_specs=[VM] * 2,
        scratch_shapes=[
            pltpu.VMEM(expert.shape, jnp.int32),
            pltpu.VMEM(weight.shape, F32),
            pltpu.VMEM((rows, rows), F32),
            pltpu.SemaphoreType.DMA((6,)),
        ],
        compiler_params=grant(8),
        name="prep",
    )(*in_hbm(x, cot, expert, weight))


def start_all(sources, targets, sems):
    copies = [
        pltpu.make_async_copy(source, target, sems.at[at])
        for at, (source, target) in enumerate(zip(sources, targets))
    ]
    for copy in copies:
        copy.start()
    return copies


def wait_for(copies, at):
    if copies:
        copies[at].wait()


def through_expert(core, half, x_ref, mix_ref, weights, ready, hid_ref, dg_ref, du_ref, mine_ref, theirs_ref, acc_ref):
    gate_ref, up_ref, down_ref = weights
    wait_for(ready, 0)
    gate = nn(x_ref[...], gate_ref[...])
    sigmoid = 1.0 / (1.0 + jnp.exp(-gate))
    active = gate * sigmoid
    wait_for(ready, 1)
    upper = nn(x_ref[...], up_ref[...])
    hid_ref[...] = (active * upper).astype(BF)
    wait_for(ready, 2)
    d_hidden = nt(mix_ref[...], down_ref[...])
    du_ref[...] = (d_hidden * active).astype(BF)
    dg_ref[...] = (d_hidden * upper * sigmoid * (1.0 + gate * (1.0 - sigmoid))).astype(BF)
    acc_ref[...] = nt(dg_ref[...], gate_ref[...]) + nt(du_ref[...], up_ref[...])
    for chunk in range(mine_ref.shape[0]):
        start = pl.multiple_of((2 * chunk + core) * half, half)
        mine_ref[chunk] = acc_ref[pl.ds(start, half), :]
        start = pl.multiple_of((2 * chunk + 1 - core) * half, half)
        theirs_ref[chunk] = acc_ref[pl.ds(start, half), :].astype(BF)


def own_kernel(x_hbm, cot_hbm, expert_hbm, weight_hbm, gate_hbm, up_hbm, down_hbm, gate_ref, up_ref, down_ref, x_ref, mix_ref, *refs):
    outs, (acc_ref, cot_ref, e_ref, w_ref, sems) = refs[:5], refs[5:]
    mine, core, _ = spot()
    half = x_ref.shape[0] // 2
    copies = start_all(
        (expert_hbm, weight_hbm, x_hbm, cot_hbm, gate_hbm, up_hbm, down_hbm),
        (e_ref, w_ref, x_ref, cot_ref, gate_ref, up_ref, down_ref),
        sems,
    )
    for copy in copies[:4]:
        copy.wait()
    column = column_of(packed_weights(e_ref, w_ref), mine)
    mix_ref[...] = (column * cot_ref[...].astype(F32)).astype(BF)
    through_expert(core, half, x_ref, mix_ref, (gate_ref, up_ref, down_ref), copies[4:], *outs, acc_ref)


def expert_outs(rows, half, width, hidden):
    chunks = rows // (2 * half)
    return (
        [jax.ShapeDtypeStruct((rows, width), BF)] * 2
        + [jax.ShapeDtypeStruct((rows, hidden), BF)] * 3
        + [jax.ShapeDtypeStruct((chunks, half, width), F32), jax.ShapeDtypeStruct((chunks, half, width), BF)]
    )


def own_rows(x, cot, expert, weight, gate_w, up_w, down_w):
    rows, width = x.shape
    inputs = (x, cot, expert, weight, gate_w, up_w, down_w)
    return pl.pallas_call(
        own_kernel,
        out_shape=[pltpu.VMEM(one.shape, one.dtype) for one in inputs[4:]]
        + expert_outs(rows, rows // 2, width, gate_w.shape[1]),
        in_specs=[HB] * 7,
        out_specs=[VM] * 10,
        scratch_shapes=[pltpu.VMEM((rows, width), F32)]
        + [pltpu.VMEM(one.shape, one.dtype) for one in inputs[1:4]]
        + [pltpu.SemaphoreType.DMA((7,))],
        compiler_params=grant(10),
        name="own_rows",
    )(*in_hbm(*inputs))


def came_kernel(half, layout, *refs):
    pieces = refs[: len(layout)]
    weights = refs[len(layout) : len(layout) + 3]
    x_ref, mix_ref, *outs = refs[len(layout) + 3 : len(layout) + 10]
    (acc_ref,) = refs[len(layout) + 10 :]
    width = x_ref.shape[1]
    mine, core, _ = spot()
    for piece, (chunk, other, at) in zip(pieces, layout):
        count = piece.shape[0]
        start = (2 * chunk + (core ^ other)) * half + at * count
        block = pl.ds(pl.multiple_of(start, count), count)
        x_ref[block, :] = piece[:, :width]
        column = column_of(piece[:, 2 * width :].astype(F32), mine)
        mix_ref[block, :] = (column * piece[:, width : 2 * width].astype(F32)).astype(BF)
    through_expert(core, half, x_ref, mix_ref, weights, (), *outs, acc_ref)


def came_rows(chunks, half, width, pieces, layout, gate_w, up_w, down_w):
    rows = 2 * half * chunks
    held = (gate_w, up_w, down_w)
    return pl.pallas_call(
        functools.partial(came_kernel, half, layout),
        out_shape=expert_outs(rows, half, width, gate_w.shape[1]),
        in_specs=[VM] * len(pieces) + [VM] * 3,
        out_specs=[VM] * 7,
        scratch_shapes=[pltpu.VMEM((rows, width), F32)],
        compiler_params=grant(14),
    )(*pieces, *in_vmem(*held))


def collect_kernel(count, *refs):
    outs = refs[-count:]
    for kind, out in enumerate(outs):
        at = 0
        for part in refs[kind : len(refs) - count : count]:
            out[at : at + part.shape[0], :] = part[...]
            at += part.shape[0]


def collect(parts):
    count = len(parts[0])
    total = sum(part[0].shape[0] for part in parts)
    return pl.pallas_call(
        functools.partial(collect_kernel, count),
        out_shape=[jax.ShapeDtypeStruct((total, one.shape[1]), one.dtype) for one in parts[0]],
        in_specs=[VM] * (count * len(parts)),
        out_specs=[VM] * count,
        compiler_params=grant(20),
        name="collect",
    )(*[one for part in parts for one in part])


def transposed_dot(a, b):
    return lax.dot_general(a, b, (((0,), (0,)), ((), ())), preferred_element_type=F32).astype(BF)


def pair_kernel(mine_ref, theirs_ref, *outs):
    for chunk, out in enumerate(outs):
        out[...] = (mine_ref[chunk] + theirs_ref[chunk].astype(F32)).astype(BF)


def paired(mine, theirs):
    chunks, half, width = mine.shape
    return pl.pallas_call(
        pair_kernel, out_shape=[jax.ShapeDtypeStruct((half, width), BF)] * chunks,
        in_specs=[VM, VM], out_specs=[VM] * chunks, compiler_params=grant(6),
    )(mine, theirs)


def split_kernel(groups, levels, own_ref, part_ref, *refs):
    got = refs[: groups - 1]
    keep_ref = refs[groups - 1]
    sends = refs[groups:]
    half = part_ref.shape[0]
    share = half // levels
    _, _, level = spot()
    for mask in range(levels):
        here = pl.ds(pl.multiple_of((level ^ mask) * share, share), share)
        total = own_ref[here, :] + part_ref[here, :].astype(F32)
        for piece in got:
            total = total + piece[here, :].astype(F32)
        if mask == 0:
            keep_ref[...] = total
        else:
            sends[mask - 1][...] = total.astype(BF)


def join_kernel(cot_ref, keep_ref, *refs):
    out_ref = refs[-1]
    _, core, level = spot()
    share = keep_ref.shape[0]
    half = cot_ref.shape[0] // 2
    start = pl.multiple_of(core * half + level * share, share)
    total = cot_ref[pl.ds(start, share), :].astype(F32) + keep_ref[...]
    for piece in refs[:-1]:
        total = total + piece[...].astype(F32)
    out_ref[...] = total.astype(BF)


def cut_kernel(levels, groups, *refs):
    blocks, (half_ref, *cuts) = refs[:levels], refs[levels:]
    mine, _, level = spot()
    share = blocks[0].shape[0]
    for mask, block in enumerate(blocks):
        half_ref[pl.ds(pl.multiple_of((level ^ mask) * share, share), share), :] = block[...]
    slab = half_ref.shape[1] // groups
    for mask, cut in enumerate(cuts):
        cut[...] = half_ref[:, pl.ds(pl.multiple_of((mine ^ mask) * slab, slab), slab)]


def exact(a, b, contract):
    return lax.dot_general(
        a, b, ((contract[:1], contract[1:]), ((), ())), precision=HIGH, preferred_element_type=F32
    )


def grown_kernel(q_ref, k_ref, decay_ref, state_ref, grown_ref, last_ref, scores_ref, turned_ref):
    spans, heads = scores_ref.shape[:2]
    at = lax.broadcasted_iota(jnp.int32, (SPAN, SPAN), 0)
    to = lax.broadcasted_iota(jnp.int32, (SPAN, SPAN), 1)
    causal = (at >= to).astype(F32)
    channel = lax.broadcasted_iota(jnp.int32, (1, q_ref.shape[1]), 1) // DK
    scale = DK ** (-0.5)
    for span in range(spans):
        here = slice(span * SPAN, (span + 1) * SPAN)
        cumulative = exact(causal, decay_ref[here, :], (1, 0))
        last = cumulative[SPAN - 1 :, :]
        last_ref[span] = jnp.broadcast_to(last, last_ref.shape[1:])
        up, down = jnp.exp(cumulative), jnp.exp(-cumulative)
        ending = jnp.exp(last - cumulative)
        keys = k_ref[here, :].astype(F32)
        grown, shrunk = q_ref[here, :].astype(F32) * up, keys * down
        for kind, value in enumerate((grown, shrunk, keys * ending, scale * up, scale * down, ending)):
            grown_ref[kind, here, :] = value
        for head in range(heads):
            own = jnp.where(channel == head, grown, 0.0)
            scores_ref[span, head] = scale * exact(own, shrunk, (1, 1)) * causal
        turned_ref[span] = state_ref[span].T


def mix_kernel(first_ref, second_ref, proj_ref, grown_ref, last_ref, mix_ref, local_ref, message_ref, both_ref):
    _, core, _ = spot()
    half = first_ref.shape[0]
    both_ref[pl.ds(pl.multiple_of(core * half, half), half), :] = first_ref[...]
    both_ref[pl.ds(pl.multiple_of((1 - core) * half, half), half), :] = second_ref[...]
    mix_ref[...] = nt(both_ref[...], proj_ref[...])
    spans, value_dim = local_ref.shape[0], local_ref.shape[1]
    channel = lax.broadcasted_iota(jnp.int32, (1, local_ref.shape[2]), 1) // DK
    heads = local_ref.shape[2] // DK
    carry = jnp.zeros(local_ref.shape[1:], F32)
    total = jnp.zeros((16, local_ref.shape[2]), F32)
    for span in reversed(range(spans)):
        here = slice(span * SPAN, (span + 1) * SPAN)
        query = grown_ref[0, here, :] * (DK ** (-0.5))
        grads = jnp.concatenate(
            [mix_ref[here, head * value_dim : (head + 1) * value_dim] for head in range(heads)], 0
        )
        queries = jnp.concatenate([jnp.where(channel == head, query, 0.0) for head in range(heads)], 0)
        local = exact(grads, queries, (0, 0))
        local_ref[span] = local
        carry = local + jnp.exp(last_ref[span][:1, :]) * carry
        total = total + last_ref[span]
    message_ref[:value_dim, :] = carry.astype(BF)
    message_ref[value_dim:, :] = jnp.exp(total).astype(BF)


def within_kernel(mix_ref, v_ref, grown_ref, scores_ref, state_ref, dq_ref, dk_ref, dv_ref):
    spans, heads = scores_ref.shape[:2]
    value_dim = v_ref.shape[1] // heads
    channel = lax.broadcasted_iota(jnp.int32, (1, heads * DK), 1) // DK
    line = lax.broadcasted_iota(jnp.int32, (heads * DK, 1), 0) // DK
    at = lax.broadcasted_iota(jnp.int32, (SPAN, SPAN), 0)
    to = lax.broadcasted_iota(jnp.int32, (SPAN, SPAN), 1)
    causal = (at >= to).astype(F32)
    for span in range(spans):
        here = slice(span * SPAN, (span + 1) * SPAN)
        query, key = grown_ref[0, here, :], grown_ref[1, here, :]
        dots = []
        for head in range(heads):
            wide = slice(head * value_dim, (head + 1) * value_dim)
            grads = mix_ref[here, wide]
            dots.append(exact(grads, v_ref[here, wide].astype(F32), (1, 1)) * causal)
            dv_ref[here, wide] = exact(scores_ref[span, head], grads, (0, 0))
        keys = jnp.concatenate([jnp.where(channel == head, key, 0.0) for head in range(heads)], 0)
        queries = jnp.concatenate([jnp.where(channel == head, query, 0.0) for head in range(heads)], 0)
        state = jnp.concatenate([jnp.where(line == head, state_ref[span], 0.0) for head in range(heads)], 1)
        dq = exact(jnp.concatenate(dots, 1), keys, (1, 0)) + exact(mix_ref[here, :], state, (1, 1))
        dq_ref[here, :] = grown_ref[3, here, :] * dq
        dk_ref[here, :] = grown_ref[4, here, :] * exact(jnp.concatenate(dots, 0), queries, (0, 0))


def final_kernel(groups, *refs):
    messages = refs[: groups - 1]
    (q_ref, k_ref, v_ref, grown_ref, last_ref, turned_ref, local_ref, dq_ref, dk_ref, dv_ref) = refs[
        groups - 1 : groups + 9
    ]
    q_out, k_out, v_out, decay_out = refs[groups + 9 :]
    mine, _, _ = spot()
    spans, value_dim, channels = local_ref.shape
    heads = channels // DK
    channel = lax.broadcasted_iota(jnp.int32, (1, channels), 1) // DK
    at = lax.broadcasted_iota(jnp.int32, (SPAN, SPAN), 0)
    to = lax.broadcasted_iota(jnp.int32, (SPAN, SPAN), 1)
    onward = (at <= to).astype(F32)
    ending = jnp.zeros((value_dim, channels), F32)
    for ahead in reversed(range(1, groups)):
        message = messages[ahead - 1][...].astype(F32)
        passed = message[:value_dim, :] + message[value_dim : value_dim + 1, :] * ending
        ending = jnp.where(mine + ahead < groups, passed, ending)
    for span in reversed(range(spans)):
        here = slice(span * SPAN, (span + 1) * SPAN)
        values = v_ref[here, :].astype(F32)
        last = jnp.exp(last_ref[span][:1, :])
        key_end = grown_ref[2, here, :]
        ends = jnp.concatenate([jnp.where(channel == head, ending, 0.0) for head in range(heads)], 0)
        through = exact(values, ends, (1, 0))
        dq = dq_ref[here, :]
        dk = dk_ref[here, :] + grown_ref[5, here, :] * through
        for head in range(heads):
            wide = slice(head * value_dim, (head + 1) * value_dim)
            own = jnp.where(channel == head, key_end, 0.0)
            v_out[here, wide] = (dv_ref[here, wide] + exact(own, ending, (1, 1))).astype(BF)
        tail = last * jnp.sum(turned_ref[span] * ending, axis=0, keepdims=True)
        tail = tail + jnp.sum(key_end * through, axis=0, keepdims=True)
        change = q_ref[here, :].astype(F32) * dq - k_ref[here, :].astype(F32) * dk
        decay_out[here, :] = exact(onward, change, (1, 0)) + tail
        q_out[here, :] = dq.astype(BF)
        k_out[here, :] = dk.astype(BF)
        ending = local_ref[span] + last * ending


def proj_kernel(groups, *refs):
    out_ref, left_ref, right_ref = refs[-3:]
    _, core, _ = spot()
    half = refs[0].shape[0]
    rows = 2 * half
    for group in range(groups):
        own, other, saved = refs[3 * group : 3 * group + 3]
        left_ref[pl.ds(pl.multiple_of(group * rows + core * half, half), half), :] = own[...]
        left_ref[pl.ds(pl.multiple_of(group * rows + (1 - core) * half, half), half), :] = other[...]
        right_ref[group * rows : (group + 1) * rows, :] = saved[...]
    out_ref[...] = lax.dot_general(
        left_ref[...], right_ref[...], (((0,), (0,)), ((), ())), preferred_element_type=F32
    )


def call(kernel, outs, args, mib, scratch=()):
    return pl.pallas_call(
        kernel, out_shape=outs, in_specs=[VM] * len(args), out_specs=[VM] * len(outs),
        scratch_shapes=scratch, compiler_params=grant(mib),
    )(*args)


def like(*shape, dtype=F32):
    return jax.ShapeDtypeStruct(shape, dtype)


def whole_rows(mesh):
    return mesh.shape["sp"] == 4 and mesh.shape["tp"] % 2 == 0


def by_rows(*args):
    return rows_on_device(*args)


def rows_on_device(
    moe_input, cotangent, route_expert, route_weight, w_gate, w_up, w_down, out_proj,
    saved_out, queries, keys, values, log_decay, span_state,
):
    rows, width = moe_input.shape
    half = rows // 2
    groups = lax.axis_size("sp")
    lanes = lax.axis_size("tp")
    levels = lanes // 2
    share = half // levels
    mine = lax.axis_index("sp").astype(jnp.int32)
    lane = lax.axis_index("tp").astype(jnp.int32)
    gate_w, up_w, down_w = w_gate[0], w_up[0], w_down[0]
    expert_t, weight_t = route_expert.T, route_weight.T

    first, second = prepare(moe_input, cotangent, expert_t, weight_t)
    x_first = swap(first, "sp", 1)
    y_second = swap(second, "sp", 2)
    x_second = swap(second, "sp", 1)
    y_first = swap(first, "sp", 2)
    gate_w, up_w, down_w, own_x, own_cot, own_hid, own_dg, own_du, own_mine, own_theirs = own_rows(
        moe_input, cotangent, expert_t, weight_t, gate_w, up_w, down_w
    )
    x_first, y_second, own_theirs, queries_then = lax.optimization_barrier(
        (x_first, y_second, own_theirs, queries)
    )
    d_first = swap(x_first, "sp", 2)
    d_second = swap(y_second, "sp", 1)
    own_part = swap(own_theirs, "tp", 1)
    channels, value_dim = queries.shape[1], values.shape[1] * DK // queries.shape[1]
    spans, heads = rows // SPAN, channels // DK
    grown, last, scores, turned = call(
        grown_kernel,
        [like(6, rows, channels), like(spans, 16, channels), like(spans, heads, SPAN, SPAN),
         like(spans, value_dim, channels)],
        (queries_then, keys, log_decay, span_state), 6,
    )
    x_second, y_first, grown = lax.optimization_barrier((x_second, y_first, grown))
    near, far = [x_first, x_second, y_first, y_second], [d_first, d_second]
    near_layout = [(chunk, other, at) for other in range(2) for chunk in range(2) for at in range(2)]
    far_layout = [(0, other, at) for other in range(2) for at in range(2)]
    near += [swap(piece, "tp", 1) for piece in near]
    near_x, near_cot, near_hid, near_dg, near_du, near_mine, near_theirs = came_rows(
        2, half, width, near, tuple(near_layout), gate_w, up_w, down_w
    )
    near_partner = swap(near_theirs, "tp", 1)
    near_back = paired(near_mine, near_partner)
    far += [swap(piece, "tp", 1) for piece in far]
    *far, near_one, near_two = lax.optimization_barrier((*far, *near_back))
    back = [swap(near_one, "sp", 1)]
    back.append(swap(near_two, "sp", 2))
    far_x, far_cot, far_hid, far_dg, far_du, far_mine, far_theirs = came_rows(
        1, half, width, far, tuple(far_layout), gate_w, up_w, down_w
    )
    (far_back,) = paired(far_mine, swap(far_theirs, "tp", 1))
    back.append(swap(far_back, "sp", 3))
    all_x, all_cot, hid, dg, du = collect(
        [
            [own_x, own_cot, own_hid, own_dg, own_du],
            [near_x, near_cot, near_hid, near_dg, near_du],
            [far_x, far_cot, far_hid, far_dg, far_du],
        ]
    )
    grad_down = transposed_dot(hid, all_cot)
    grad_gate = transposed_dot(all_x, dg)
    *back, grad_down, grad_gate = lax.optimization_barrier((*back, grad_down, grad_gate))
    small = jax.ShapeDtypeStruct((share, width), BF)
    keep, *outgoing = pl.pallas_call(
        functools.partial(split_kernel, groups, levels),
        out_shape=[jax.ShapeDtypeStruct((share, width), F32)] + [small] * (levels - 1),
        in_specs=[VM] * (groups + 1), out_specs=[VM] * levels, name="split", compiler_params=grant(6),
    )(own_mine[0], own_part[0], *back)
    incoming = []
    for mask, piece in enumerate(outgoing):
        incoming.append(swap(piece, "tp", 2 * (mask + 1)))
    grad_up = transposed_dot(all_x, du)
    keep, saved_send = lax.optimization_barrier((keep, saved_out))
    saved_all = [saved_out]
    for mask in range(1, groups):
        saved_all.append(swap(saved_send, "sp", mask))
    (block,) = call(join_kernel, [small], (cotangent, keep, *incoming), 6)
    blocks = [block]
    for mask in range(1, levels):
        blocks.append(swap(block, "tp", 2 * mask))
    *blocks, grad_up = lax.optimization_barrier((*blocks, grad_up))
    slab = width // groups
    this_half, *cuts = call(
        functools.partial(cut_kernel, levels, groups),
        [like(half, width, dtype=BF)] + [like(half, slab, dtype=BF)] * groups, blocks, 6,
    )
    other_half = swap(this_half, "tp", 1)
    got_cuts = [cuts[0]]
    for mask in range(1, groups):
        got_cuts.append(swap(cuts[mask], "sp", mask))

    mix, local, message = call(
        mix_kernel,
        [like(rows, heads * value_dim), like(spans, value_dim, channels), like(value_dim + 16, channels, dtype=BF)],
        (this_half, other_half, out_proj, grown, last), 8,
        [pltpu.VMEM((rows, width), BF)],
    )
    messages = []
    for ahead in range(1, groups):
        messages.append(lax.ppermute(message, "sp", [(i, i - ahead) for i in range(ahead, groups)]))
    dq, dk, dv = call(
        within_kernel, [like(rows, channels)] * 2 + [like(rows, heads * value_dim)],
        (mix, values, grown, scores, span_state), 6,
    )
    *got_cuts, dq = lax.optimization_barrier((*got_cuts, dq))
    parts = []
    for mask in range(groups):
        parts += [got_cuts[mask], swap(got_cuts[mask], "tp", 1), saved_all[mask]]
    (grad_proj,) = call(
        functools.partial(proj_kernel, groups), [like(slab, saved_out.shape[1])], parts, 8,
        [pltpu.VMEM((groups * rows, slab), BF), pltpu.VMEM((groups * rows, saved_out.shape[1]), BF)],
    )
    grad_queries, grad_keys, grad_values, grad_decay = call(
        functools.partial(final_kernel, groups),
        [like(rows, channels, dtype=BF)] * 2 + [like(rows, heads * value_dim, dtype=BF), like(rows, channels)],
        (*messages, queries, keys, values, grown, last, turned, local, dq, dk, dv), 8,
    )
    return (
        grad_gate[None], grad_up[None], grad_down[None], grad_proj,
        grad_queries, grad_keys, grad_values, grad_decay,
    )


def solution(mesh):
    placed = (
        P("sp", None), P("sp", None), P("sp", None), P("sp", None),
        P("sp", None, "tp"), P("sp", None, "tp"), P("sp", "tp", None),
        P("tp", None), P("sp", "tp"), P("sp", "tp"), P("sp", "tp"),
        P("sp", "tp"), P("sp", "tp"), P("sp", "tp", None),
    )
    return jax.shard_map(
        by_rows if whole_rows(mesh) else by_slots,
        mesh=mesh,
        in_specs=placed,
        out_specs=(
            P("sp", None, "tp"), P("sp", None, "tp"), P("sp", "tp", None),
            P("sp", "tp"), P("sp", "tp"), P("sp", "tp"), P("sp", "tp"), P("sp", "tp"),
        ),
        check_vma=False,
    )
```
